512 devices in a mesh: grp: 2 (over y), kv: 32 (over z), tp: 8 (over x, core).
Axes of the slice: x: 4, y: 2, z: 32, core: 2. Of those that a mesh axis runs over, the one named last changes fastest.
The devices are a block of a 4x8x32 slice.
Arguments:
- tokens: bfloat16 [48, 4096], P('grp', ('kv', 'tp')), parts along dimension 0, may hold values from -12 to 12
- lengths: int32 [48], P('grp'), parts along dimension 0, may hold values from 1 to 1024, 12288 in all
- attn_gain: float32 [4096], P('kv'), may hold values from 0.1 to 1.9
- w_query: bfloat16 [4096, 4096], P('kv', 'tp'), may hold values from -0.09375 to 0.09375
- w_key: bfloat16 [4096, 4096], P('kv', 'tp'), may hold values from -0.09375 to 0.09375
- w_value: bfloat16 [4096, 4096], P('kv', 'tp'), may hold values from -0.09375 to 0.09375
- w_gate: bfloat16 [4096, 4096], P('kv', 'tp'), may hold values from -0.09375 to 0.09375
- log_decay: float32 [16], P('tp'), may hold values from -1 to 0
- key_cache: bfloat16 [48, 1024, 4096], P('grp', 'kv', 'tp'), parts along dimension 0, may hold values from -6 to 6
- value_cache: bfloat16 [48, 1024, 4096], P('grp', 'kv', 'tp'), parts along dimension 0, may hold values from -6 to 6
- gn_gain: float32 [4096], P('tp'), may hold values from 0.1 to 1.9
- w_out: bfloat16 [4096, 4096], P('tp', 'kv'), may hold values from -0.1875 to 0.1875
- ffn_gain: float32 [4096], P('kv'), may hold values from 0.1 to 1.9
- w_ffn_gate: bfloat16 [4096, 11264], P('kv', 'tp'), may hold values from -0.09375 to 0.09375
- w_ffn_up: bfloat16 [4096, 11264], P('kv', 'tp'), may hold values from -0.09375 to 0.09375
- w_ffn_down: bfloat16 [11264, 4096], P('tp', 'kv'), may hold values from -0.109375 to 0.109375
Outputs:
- layer_out: bfloat16 [48, 4096], P('grp', ('kv', 'tp')), parts along dimension 0
The draws below stay inside these ranges and needn't reach their ends.
There are 2 independent parts, one for each index of `grp`. The reference program is written for one: setup_inputs(seed, part) draws one part's arguments, and reference() takes and returns one part's arrays. A program takes and returns all parts, laid end to end along the dimension named above; an argument that names none is the same for every part. Nothing has to cross between parts.
All inputs are finite; a program needn't handle non-finite values.
Results may differ from the reference program's by a relative error of at most 0.012.
Values may be sent and summed in bfloat16 or wider, within the bound.
No kernel may reach another device: no remote copies, remote signals or barrier semaphores. Data moves between devices by JAX's collectives and lax.ppermute only.
A program may use at most 64 MiB of HBM per device.

```python
import math
import jax
import jax.numpy as jnp
import numpy as np
from jax import lax

HEADS = 16
DK = 256
FF = 11264
SEQS = 24
D = 4096
L_CACHE = 1024
N_KV = 32


def draw_tokens(key, part):
    folded = jax.random.fold_in(key, 11)
    second_key = jax.random.fold_in(folded, 0)
    ramp = jnp.arange(N_KV, dtype=jnp.float32) / (N_KV - 1)
    block_scale = jnp.exp(ramp * 1.0986)
    entries = jnp.clip(jax.random.normal(second_key, (SEQS, D), jnp.float32), -4.0, 4.0)
    col_scale = jnp.repeat(block_scale, D // N_KV)
    return (entries * col_scale[None, :]).astype(jnp.bfloat16)


def draw_log_decay(key, part):
    folded = jax.random.fold_in(key, 23)
    pick_key, slow_key, fast_key = jax.random.split(folded, 3)
    slow_share = 0.5
    picked = jax.random.uniform(pick_key, (HEADS,), jnp.float32) < slow_share
    slow_rate = -2.3 * jax.random.uniform(slow_key, (HEADS,), jnp.float32, 0.3, 1.0) / L_CACHE
    fast_rate = -1.0 / jax.random.uniform(fast_key, (HEADS,), jnp.float32, 30.0, 60.0)
    return jnp.where(picked, slow_rate, fast_rate).astype(jnp.float32)


def levels(rng, dims, cuts, smallest, top_value):
    gain = 1.0
    for dim, parts in cuts:
        heights = jax.random.uniform(jax.random.fold_in(jax.random.fold_in(rng, 6), dim), (parts,), jnp.float32, smallest / len(cuts), top_value / len(cuts))
        gain = gain * jnp.repeat(jnp.exp(heights), dims[dim] // parts).reshape((-1,) + (1,) * (len(dims) - 1 - dim))
    return gain


def split_up(count, total, limit, skew):
    portions = [(1 << 20) // math.isqrt(rank ** skew) + 1 for rank in range(2, count + 1)]
    spare, holding = total - limit - (count - 1), [1] * (count - 1)
    while spare > 0:
        free = [i for i in range(count - 1) if holding[i] < limit]
        pool, left = sum([portions[i] for i in free]), spare
        for i in free:
            more = min(limit - holding[i], max(1, left * portions[i] // pool), spare)
            holding[i] = holding[i] + more
            spare = spare - more
    return np.array([limit] + holding)


def uneven_parts(key, count, total, reach, slope):
    if count == 2:
        one = jax.random.randint(key, (), max(1, total - reach), min(reach, total - 1) + 1)
        return jnp.stack([one, total - one])
    sizes = jnp.asarray(split_up(count, total, reach, slope), jnp.int32)
    twos = (count - 1) // 2
    giver, taker = sizes[1:1 + 2 * twos:2], sizes[2:2 + 2 * twos:2]
    margin = jnp.minimum(giver - 1, reach - taker)
    moved = jax.random.randint(jax.random.fold_in(key, 1), (twos,), 0, 1 << 20) % (margin + 1)
    sizes = sizes.at[1:1 + 2 * twos:2].set(giver - moved).at[2:2 + 2 * twos:2].set(taker + moved)
    return sizes[jax.random.permutation(jax.random.fold_in(key, 2), count)]


def centred(stream_key, shape, scale, limit, pieces=(), kind=jnp.bfloat16):
    array = scale * jax.random.normal(stream_key, shape, jnp.float32)
    if pieces:
        array = array * levels(stream_key, shape, pieces, -0.22, 0.18)
    return jnp.clip(array, -limit, limit).astype(kind)


def setup_inputs(seed: int = 0, part: int = 0) -> dict:
    splits = jax.random.split(jax.random.key(seed), 17)
    own_keys = jax.random.split(jax.random.fold_in(splits[16], part), 17)
    return {
        "tokens": draw_tokens(jax.random.fold_in(jax.random.fold_in(splits[16], part), 71), part),
        "lengths": uneven_parts(own_keys[1], SEQS, SEQS * L_CACHE // 2, L_CACHE, 2).astype(jnp.int32),
        "attn_gain": jnp.clip(1.0 + 0.18 * jax.random.normal(splits[2], (D,), jnp.float32), 0.1, 1.9),
        "w_query": centred(splits[3], (D, D), D ** -0.5, 0.09375, ((0, 32), (1, 8))),
        "w_key": centred(splits[4], (D, D), D ** -0.5, 0.09375, ((0, 32), (1, 8))),
        "w_value": centred(splits[5], (D, D), D ** -0.5, 0.09375, ((0, 32), (1, 8))),
        "w_gate": centred(splits[6], (D, D), D ** -0.5, 0.09375, ((0, 32), (1, 8))),
        "log_decay": draw_log_decay(jax.random.fold_in(splits[16], 71), part),
        "key_cache": centred(own_keys[8], (SEQS, L_CACHE, D), 1.0, 6.0, ((1, 32), (2, 8))),
        "value_cache": centred(own_keys[9], (SEQS, L_CACHE, D), 1.0, 6.0, ((1, 32), (2, 8))),
        "gn_gain": jnp.clip(1.0 + 0.18 * jax.random.normal(splits[10], (D,), jnp.float32), 0.1, 1.9),
        "w_out": centred(splits[11], (D, D), (D // 4) ** -0.5, 0.1875, ((0, 8), (1, 32))),
        "ffn_gain": jnp.clip(1.0 + 0.18 * jax.random.normal(splits[12], (D,), jnp.float32), 0.1, 1.9),
        "w_ffn_gate": centred(splits[13], (D, FF), D ** -0.5, 0.09375, ((0, 32), (1, 8))),
        "w_ffn_up": centred(splits[14], (D, FF), D ** -0.5, 0.09375, ((0, 32), (1, 8))),
        "w_ffn_down": centred(splits[15], (FF, D), (FF // 4) ** -0.5, 0.109375, ((0, 8), (1, 32))),
    }


RMS_EPS = 0.1
GN_EPS = 1.0
ROPE_BASE = 10000.0

def rotate(vectors, positions):
    half_dim = vectors.shape[-1] // 2
    inverse = ROPE_BASE ** (-jnp.arange(half_dim, dtype=jnp.float32) / half_dim)
    angles = positions[:, None, None] * inverse[None, None, :]
    cosine = jnp.cos(angles)
    sine_part = jnp.sin(angles)
    front_part = vectors[..., :half_dim]
    back_part = vectors[..., half_dim:]
    return jnp.concatenate([front_part * cosine - back_part * sine_part, front_part * sine_part + back_part * cosine], axis=-1)

def group_norm(totals, gn_gain):
    width = totals.shape[-1]
    center = lax.optimization_barrier(jnp.sum(totals, axis=-1, keepdims=True)) / width
    spread = lax.optimization_barrier(jnp.sum(totals * totals, axis=-1, keepdims=True)) / width - center * center
    normed = (totals - center) * lax.rsqrt(spread + GN_EPS)
    return normed.reshape(normed.shape[0], -1) * gn_gain

def reference(tokens, lengths, attn_gain, w_query, w_key, w_value, w_gate, log_decay, key_cache, value_cache, gn_gain, w_out, ffn_gain, w_ffn_gate, w_ffn_up, w_ffn_down):
    batch_rows = tokens.shape[0]
    heads_all = log_decay.shape[0]
    widened = tokens.astype(jnp.float32)
    factor = lax.rsqrt(lax.optimization_barrier(jnp.sum(widened * widened, axis=1)) / D + RMS_EPS)[:, None]
    scaled = (widened * attn_gain).astype(jnp.bfloat16)
    queries = jnp.dot(scaled, w_query, preferred_element_type=jnp.float32) * factor
    new_keys = jnp.dot(scaled, w_key, preferred_element_type=jnp.float32) * factor
    new_values = jnp.dot(scaled, w_value, preferred_element_type=jnp.float32) * factor
    gates = jnp.dot(scaled, w_gate, preferred_element_type=jnp.float32) * factor
    positions = lengths.astype(jnp.float32)
    queries = rotate(queries.reshape(batch_rows, heads_all, DK), positions) * DK ** (-0.5)
    new_keys = rotate(new_keys.reshape(batch_rows, heads_all, DK), positions)
    new_values = new_values.reshape(batch_rows, heads_all, DK)
    query_low = queries.astype(jnp.bfloat16)
    cache_len = key_cache.shape[1]
    slots = jnp.arange(cache_len, dtype=jnp.int32)

    def one_sequence(packed):
        keys_seq, values_seq, query_seq, length = packed
        keys_wide = keys_seq.astype(jnp.float32).reshape(cache_len, heads_all, DK)
        scores = jnp.einsum('phd,hd->ph', keys_wide, query_seq.astype(jnp.float32))
        gaps = (length - slots).astype(jnp.float32)
        decays = jnp.exp(log_decay[None, :] * jnp.maximum(gaps, 0.0)[:, None])
        mixing = jnp.where((slots < length)[:, None], scores * decays, 0.0).astype(jnp.bfloat16)
        values_wide = values_seq.astype(jnp.float32).reshape(cache_len, heads_all, DK)
        return jnp.einsum('ph,phd->hd', mixing.astype(jnp.float32), values_wide)
    cached = lax.map(one_sequence, (key_cache, value_cache, query_low, lengths.astype(jnp.int32)))
    own_term = lax.optimization_barrier(jnp.sum(queries * new_keys, axis=-1, keepdims=True)) * new_values
    normed = group_norm(cached + own_term, gn_gain)
    gated = (jax.nn.silu(gates) * normed).astype(jnp.bfloat16)
    mixed = jnp.dot(gated, w_out, preferred_element_type=jnp.float32)
    resid = (widened + mixed).astype(jnp.bfloat16)
    resid_wide = resid.astype(jnp.float32)
    factor_mid = lax.rsqrt(lax.optimization_barrier(jnp.sum(resid_wide * resid_wide, axis=1)) / D + RMS_EPS)[:, None]
    scaled_mid = (resid_wide * ffn_gain).astype(jnp.bfloat16)
    gate_mid = jnp.dot(scaled_mid, w_ffn_gate, preferred_element_type=jnp.float32) * factor_mid
    up_mid = jnp.dot(scaled_mid, w_ffn_up, preferred_element_type=jnp.float32) * factor_mid
    hidden = (jax.nn.silu(gate_mid) * up_mid).astype(jnp.bfloat16)
    down = jnp.dot(hidden, w_ffn_down, preferred_element_type=jnp.float32)
    return (resid_wide + down).astype(jnp.bfloat16)
```

```python
import jax
import jax.numpy as jnp
from jax import lax
from jax.sharding import PartitionSpec as P

DK = 256
D = 4096
LANES = 128
NEAR = 4

RMS_EPS = 0.1
GN_EPS = 1.0
ROPE_BASE = 10000.0


def groups_near():
    n = lax.axis_size("kv")
    return [list(range(i, i + NEAR)) for i in range(0, n, NEAR)]


def groups_far():
    n = lax.axis_size("kv")
    return [list(range(i, n, NEAR)) for i in range(NEAR)]


def exchange(blocks, axis, groups=None):
    return lax.all_to_all(
        blocks, axis, split_axis=0, concat_axis=0, tiled=True, axis_index_groups=groups
    )


def spread(array, axis, peers, groups=None):
    return exchange(jnp.broadcast_to(array, (peers, *array.shape)), axis, groups)


def wide_sum(blocks):
    return jnp.sum(blocks.astype(jnp.float32), axis=0)


def hi_lo_rows(vector):
    high = lax.reduce_precision(vector, 8, 7)
    rows = jnp.stack([high, vector - high])
    return jnp.pad(rows, ((0, 6), (0, LANES - vector.shape[0])))


def near_blocks(array):
    return jnp.stack(
        [array[:, i * LANES : (i + 1) * LANES] for i in range(array.shape[1] // LANES)]
    )


def side(blocks):
    return jnp.concatenate([blocks[i] for i in range(blocks.shape[0])], axis=1)


def reduce_pair(first, second, extra=None):
    far = lax.axis_size("kv") // NEAR
    rows = first.shape[0]
    blocks = jnp.concatenate([near_blocks(first), near_blocks(second)], axis=1)
    if extra is not None:
        tail = jnp.broadcast_to(hi_lo_rows(extra), (NEAR, 8, LANES))
        blocks = jnp.concatenate([blocks, tail], axis=1)
    got = wide_sum(exchange(blocks.astype(jnp.bfloat16), "kv", groups_near()))
    if extra is not None:
        vector = got[2 * rows] + got[2 * rows + 1]
        got = jnp.concatenate([got[: 2 * rows], hi_lo_rows(vector[: extra.shape[0]])], axis=0)
    got = wide_sum(spread(got.astype(jnp.bfloat16), "kv", far, groups_far()))
    whole = spread(got[: 2 * rows].astype(jnp.bfloat16), "kv", NEAR, groups_near())
    outs = (
        side(whole[:, :rows]).astype(jnp.float32),
        side(whole[:, rows:]).astype(jnp.float32),
    )
    if extra is None:
        return outs
    return (*outs, (got[2 * rows] + got[2 * rows + 1])[: extra.shape[0]])


def rotate(vectors, cosine, sine):
    half = DK // 2
    outs = []
    for h in range(vectors.shape[1] // DK):
        a = vectors[:, h * DK : h * DK + half]
        b = vectors[:, h * DK + half : (h + 1) * DK]
        outs += [a * cosine - b * sine, a * sine + b * cosine]
    return jnp.concatenate(outs, axis=1)


def cache_partial(query_low, lengths, log_decay, key_cache, value_cache, heads_here):
    batch_rows = query_low.shape[0]
    span = key_cache.shape[1]
    slots = lax.axis_index("kv") * span + jnp.arange(span, dtype=jnp.int32)
    live = slots[None, :] < lengths[:, None]
    gaps = jnp.maximum((lengths[:, None] - slots[None, :]).astype(jnp.float32), 0.0)
    decays = jnp.exp(log_decay[None, None, :] * gaps[:, :, None])
    keys_here = key_cache.reshape(batch_rows, span, heads_here, DK)
    values_here = value_cache.reshape(batch_rows, span, heads_here, DK)
    scores = jnp.einsum("bphd,bhd->bph", keys_here, query_low, preferred_element_type=jnp.float32)
    mixing = jnp.where(live[:, :, None], scores * decays, 0.0).astype(jnp.bfloat16)
    return jnp.einsum("bph,bphd->bhd", mixing, values_here, preferred_element_type=jnp.float32)


def local(
    tokens,
    lengths,
    attn_gain,
    w_query,
    w_key,
    w_value,
    w_gate,
    log_decay,
    key_cache,
    value_cache,
    gn_gain,
    w_out,
    ffn_gain,
    w_ffn_gate,
    w_ffn_up,
    w_ffn_down,
):
    rows = tokens.shape[0]
    heads_here = log_decay.shape[0]
    kv = lax.axis_size("kv")
    tp = lax.axis_size("tp")
    own_width = tokens.shape[1]
    gathered = spread(tokens, "tp", tp)
    x = jnp.moveaxis(gathered, 0, 1).reshape(rows, tp * own_width).astype(jnp.float32)
    own_squares = jnp.sum(x * x, axis=1)
    scaled = (x * attn_gain).astype(jnp.bfloat16)
    dot = lambda a, w: jnp.dot(a, w, preferred_element_type=jnp.float32)
    q_raw, k_raw, squares = reduce_pair(dot(scaled, w_query), dot(scaled, w_key), own_squares)
    factor = lax.rsqrt(squares / D + RMS_EPS)[:, None]
    positions = lengths.astype(jnp.float32)
    half = DK // 2
    inverse = ROPE_BASE ** (-jnp.arange(half, dtype=jnp.float32) / half)
    angles = positions[:, None] * inverse[None, :]
    cosine, sine = jnp.cos(angles), jnp.sin(angles)
    queries = rotate(q_raw * factor, cosine, sine) * DK ** (-0.5)
    keys = rotate(k_raw * factor, cosine, sine)
    by_head = (rows, heads_here, DK)
    own_dot = jnp.sum((queries * keys).reshape(by_head), axis=-1, keepdims=True)
    cached = cache_partial(
        queries.astype(jnp.bfloat16).reshape(by_head),
        lengths,
        log_decay,
        key_cache,
        value_cache,
        heads_here,
    )
    part_value = dot(scaled, w_value) * factor
    totals = cached + own_dot * part_value.reshape(by_head)
    totals = totals - jnp.mean(totals, axis=-1, keepdims=True)
    part_gate = dot(scaled, w_gate) * factor
    totals, gates = reduce_pair(totals.reshape(rows, heads_here * DK), part_gate)
    totals = totals.reshape(by_head)
    center = jnp.mean(totals, axis=-1, keepdims=True)
    spread_ = jnp.mean(totals * totals, axis=-1, keepdims=True) - center * center
    normed = ((totals - center) * lax.rsqrt(spread_ + GN_EPS)).reshape(rows, heads_here * DK)
    gated = (jax.nn.silu(gates) * (normed * gn_gain)).astype(jnp.bfloat16)
    mixed = wide_sum(spread(dot(gated, w_out).astype(jnp.bfloat16), "tp", tp))
    resid = (x + mixed).astype(jnp.bfloat16)
    resid_wide = resid.astype(jnp.float32)
    mid_squares = jnp.sum(resid_wide * resid_wide, axis=1)
    scaled_mid = (resid_wide * ffn_gain).astype(jnp.bfloat16)
    gate_part = dot(scaled_mid, w_ffn_gate)
    up_part = dot(scaled_mid, w_ffn_up)
    wide = gate_part.shape[1]
    share = wide // kv

    def for_peers(a):
        return jnp.moveaxis(a.reshape(rows, kv, share), 1, 0).reshape(kv, rows * share)

    high = lax.reduce_precision(mid_squares, 8, 7)
    stat = jnp.broadcast_to(jnp.concatenate([high, mid_squares - high]), (kv, 2 * rows))
    flat = jnp.concatenate([for_peers(gate_part), for_peers(up_part), stat], axis=1)
    size = flat.shape[1]
    flat = jnp.pad(flat, ((0, 0), (0, -size % LANES))).astype(jnp.bfloat16)
    got = wide_sum(exchange(flat, "kv"))
    gate_share = got[: rows * share].reshape(rows, share)
    up_share = got[rows * share : 2 * rows * share].reshape(rows, share)
    total_mid = got[2 * rows * share : 2 * rows * share + rows]
    total_mid = total_mid + got[2 * rows * share + rows : size]
    factor_mid = lax.rsqrt(total_mid / D + RMS_EPS)[:, None]
    hidden_share = (jax.nn.silu(gate_share * factor_mid) * (up_share * factor_mid)).astype(
        jnp.bfloat16
    )
    hidden = jnp.moveaxis(spread(hidden_share, "kv", kv), 0, 1).reshape(rows, wide)
    down_part = dot(hidden, w_ffn_down).astype(jnp.bfloat16)
    down = wide_sum(
        exchange(jnp.moveaxis(down_part.reshape(rows, tp, own_width), 1, 0), "tp")
    )
    own_at = lax.axis_index("tp") * own_width
    own_resid = lax.dynamic_slice_in_dim(resid_wide, own_at, own_width, 1)
    return (own_resid + down).astype(jnp.bfloat16)


def solution(mesh):
    return jax.shard_map(
        local,
        mesh=mesh,
        in_specs=(
            P("grp", ("kv", "tp")),
            P("grp"),
            P("kv"),
            P("kv", "tp"),
            P("kv", "tp"),
            P("kv", "tp"),
            P("kv", "tp"),
            P("tp"),
            P("grp", "kv", "tp"),
            P("grp", "kv", "tp"),
            P("tp"),
            P("tp", "kv"),
            P("kv"),
            P("kv", "tp"),
            P("kv", "tp"),
            P("tp", "kv"),
        ),
        out_specs=P("grp", ("kv", "tp")),
        check_vma=False,
    )
```

```python
import jax
import jax.numpy as jnp
from jax import lax
from jax.experimental import pallas as pl
from jax.experimental.pallas import tpu as pltpu
from jax.sharding import PartitionSpec as P

DK = 256
D = 4096
LANES = 128
NEAR = 4
F32 = jnp.float32
BF16 = jnp.bfloat16

RMS_EPS = 0.1
GN_EPS = 1.0
ROPE_BASE = 10000.0


def groups_near():
    n = lax.axis_size("kv")
    return [list(range(i, i + NEAR)) for i in range(0, n, NEAR)]


def groups_far():
    n = lax.axis_size("kv")
    return [list(range(i, n, NEAR)) for i in range(NEAR)]


def exchange(blocks, axis, groups=None):
    return lax.all_to_all(
        blocks, axis, split_axis=0, concat_axis=0, tiled=True, axis_index_groups=groups
    )


def spread(array, axis, peers, groups=None):
    return exchange(jnp.broadcast_to(array, (peers, *array.shape)), axis, groups)


def wide_sum(blocks):
    return jnp.sum(blocks.astype(F32), axis=0)


def side(blocks):
    return jnp.concatenate([blocks[i] for i in range(blocks.shape[0])], axis=1)


def kernel(body, outs, *args, scratch=(), scalars=0):
    vmem = pl.BlockSpec(memory_space=pltpu.VMEM)
    smem = pl.BlockSpec(memory_space=pltpu.SMEM)
    return pl.pallas_call(
        body,
        out_shape=outs,
        in_specs=[smem] * scalars + [vmem] * (len(args) - scalars),
        out_specs=jax.tree.map(lambda _: vmem, outs),
        scratch_shapes=list(scratch),
    )(*args)


def iota(shape, dim):
    return lax.broadcasted_iota(jnp.int32, shape, dim)


def mm(a, b):
    return jnp.dot(a, b, preferred_element_type=F32)


def column_to_row(column):
    shape = (column.shape[0], LANES)
    return jnp.sum(
        jnp.where(iota(shape, 0) == iota(shape, 1), column, 0.0), axis=0, keepdims=True
    )


def place_body(at, tokens, out):
    peers, rows, _ = out.shape
    width = tokens.shape[1]
    shape = (width, LANES)
    pick = jnp.where(iota(shape, 1) == iota(shape, 0) + at[0] * width, 1.0, 0.0).astype(BF16)
    placed = mm(tokens[...], pick).astype(BF16)
    for i in range(peers):
        out[i] = placed


def project_body(parts, gain, w_query, w_key, w_value, w_gate, blocks, value, gate, x_out):
    peers, rows, _ = parts.shape
    x = parts[0].astype(F32)
    for i in range(1, peers):
        x = x + parts[i].astype(F32)
    x_out[...] = x
    squares = column_to_row(jnp.sum(x * x, axis=1, keepdims=True))
    high = squares.astype(BF16).astype(F32)
    at = iota((8, LANES), 0)
    tail = jnp.where(at == 0, high, jnp.where(at == 1, squares - high, 0.0)).astype(BF16)
    scaled = (x * gain[...]).astype(BF16)
    query = mm(scaled, w_query[...])
    key = mm(scaled, w_key[...])
    for n in range(NEAR):
        lanes = slice(n * LANES, (n + 1) * LANES)
        blocks[n, 0:rows, :] = query[:, lanes].astype(BF16)
        blocks[n, rows : 2 * rows, :] = key[:, lanes].astype(BF16)
        blocks[n, 2 * rows : 2 * rows + 8, :] = tail
    value[...] = mm(scaled, w_value[...])
    gate[...] = mm(scaled, w_gate[...])


def mix_body(blocks, gain, w_out, out):
    peers, rows, _ = out.shape
    mixed = jnp.zeros((rows, LANES), F32)
    for h in range(NEAR // 2):
        a, b = (blocks[n, 0:rows, :].astype(F32) for n in (2 * h, 2 * h + 1))
        center = (
            jnp.sum(a, axis=1, keepdims=True) + jnp.sum(b, axis=1, keepdims=True)
        ) / DK
        a, b = a - center, b - center
        spread_ = (
            jnp.sum(a * a, axis=1, keepdims=True) + jnp.sum(b * b, axis=1, keepdims=True)
        ) / DK
        scale = lax.rsqrt(spread_ + GN_EPS)
        for n, half in ((2 * h, a), (2 * h + 1, b)):
            lanes = slice(n * LANES, (n + 1) * LANES)
            gates = blocks[n, rows : 2 * rows, :].astype(F32)
            silu = gates / (1.0 + jnp.exp(-gates))
            gated = (silu * (half * scale * gain[:, lanes])).astype(BF16)
            mixed = mixed + mm(gated, w_out[lanes, :])
    mixed = mixed.astype(BF16)
    for i in range(peers):
        out[i] = mixed


def ffn_in_body(x, parts, gain, w_gate, w_up, blocks, resid_out, gate_s, up_s, pack_s):
    peers, rows, _ = parts.shape
    wide = w_gate.shape[1]
    cuts = wide // LANES
    own = rows // NEAR
    mixed = parts[0].astype(F32)
    for i in range(1, peers):
        mixed = mixed + parts[i].astype(F32)
    resid = (x[...] + mixed).astype(BF16)
    resid_out[...] = resid
    resid = resid.astype(F32)
    squares = jnp.sum(resid * resid, axis=1, keepdims=True)
    scaled = (resid * gain[...]).astype(BF16)
    gate_s[...] = mm(scaled, w_gate[...])
    up_s[...] = mm(scaled, w_up[...])
    stat = 2 * cuts * own
    at = iota((rows, LANES), 0)
    lane = iota((rows, LANES), 1)
    for n in range(NEAR):
        for c in range(cuts):
            lanes = slice(c * LANES, (c + 1) * LANES)
            pack_s[n, c * own : (c + 1) * own, :] = gate_s[n * own : (n + 1) * own, lanes]
            pack_s[n, (cuts + c) * own : (cuts + c + 1) * own, :] = up_s[
                n * own : (n + 1) * own, lanes
            ]
        row = jnp.sum(jnp.where(at == lane + n * own, squares, 0.0), axis=0, keepdims=True)
        keep = iota((1, LANES), 1) < own
        row = jnp.where(keep, row, 0.0)
        pack_s[n, stat : pack_s.shape[1], :] = jnp.broadcast_to(
            row, (pack_s.shape[1] - stat, LANES)
        )
    blocks[...] = pack_s[...].astype(BF16)


def hidden_body(arrived, out, sum_s, *, own, cuts):
    total = arrived[0].astype(F32)
    for i in range(1, arrived.shape[0]):
        total = total + arrived[i].astype(F32)
    sum_s[...] = total
    half = own * cuts
    padded = out.shape[1]
    row = sum_s[2 * half : 2 * half + 1, :]
    shape = (padded, LANES)
    row_at = lax.rem(iota(shape, 0), own)
    squares = jnp.sum(jnp.where(row_at == iota(shape, 1), row, 0.0), axis=1, keepdims=True)
    factor = lax.rsqrt(squares / D + RMS_EPS)[0:half]
    gate = sum_s[0:half, :] * factor
    up = sum_s[half : 2 * half, :] * factor
    hidden = gate / (1.0 + jnp.exp(-gate)) * up
    for i in range(out.shape[0]):
        out[i, 0:half, :] = hidden.astype(BF16)
        if padded > half:
            out[i, half:padded, :] = jnp.zeros((padded - half, LANES), BF16)


def down_body(arrived, w_down, out, wide_s, row_s):
    peers, rows, _ = out.shape
    own = rows // NEAR
    cuts = w_down.shape[0] // LANES
    for n in range(NEAR):
        wide_s[n] = arrived[n].astype(F32)
    for c in range(cuts):
        for n in range(NEAR):
            row_s[n * own : (n + 1) * own, c * LANES : (c + 1) * LANES] = wide_s[
                n, c * own : (c + 1) * own, :
            ]
    down = mm(row_s[...].astype(BF16), w_down[...]).astype(BF16)
    for i in range(peers):
        out[i] = down


def last_body(at, arrived, resid, out):
    width = out.shape[1]
    down = arrived[0].astype(F32)
    for i in range(1, arrived.shape[0]):
        down = down + arrived[i].astype(F32)
    whole = (resid[...].astype(F32) + down).astype(BF16)
    shape = (LANES, width)
    pick = jnp.where(iota(shape, 0) == iota(shape, 1) + at[0] * width, 1.0, 0.0).astype(BF16)
    out[...] = mm(whole, pick).astype(BF16)


def rotate(vectors, cosine, sine):
    half = DK // 2
    outs = []
    for h in range(vectors.shape[1] // DK):
        a = vectors[:, h * DK : h * DK + half]
        b = vectors[:, h * DK + half : (h + 1) * DK]
        outs += [a * cosine - b * sine, a * sine + b * cosine]
    return jnp.concatenate(outs, axis=1)


def cache_partial(query_low, lengths, log_decay, key_cache, value_cache, heads_here):
    batch_rows = query_low.shape[0]
    span = key_cache.shape[1]
    slots = lax.axis_index("kv") * span + jnp.arange(span, dtype=jnp.int32)
    live = slots[None, :] < lengths[:, None]
    gaps = jnp.maximum((lengths[:, None] - slots[None, :]).astype(F32), 0.0)
    decays = jnp.exp(log_decay[None, None, :] * gaps[:, :, None])
    keys_here = key_cache.reshape(batch_rows, span, heads_here, DK)
    values_here = value_cache.reshape(batch_rows, span, heads_here, DK)
    scores = jnp.einsum("bphd,bhd->bph", keys_here, query_low, preferred_element_type=F32)
    mixing = jnp.where(live[:, :, None], scores * decays, 0.0).astype(BF16)
    return jnp.einsum("bph,bphd->bhd", mixing, values_here, preferred_element_type=F32)


def local(
    tokens,
    lengths,
    attn_gain,
    w_query,
    w_key,
    w_value,
    w_gate,
    log_decay,
    key_cache,
    value_cache,
    gn_gain,
    w_out,
    ffn_gain,
    w_ffn_gate,
    w_ffn_up,
    w_ffn_down,
):
    shape = jax.ShapeDtypeStruct
    rows = tokens.shape[0]
    heads_here = log_decay.shape[0]
    width = heads_here * DK
    kv = lax.axis_size("kv")
    tp = lax.axis_size("tp")
    far = kv // NEAR
    own = rows // NEAR
    at = lax.axis_index("tp").astype(jnp.int32).reshape(1)

    placed = kernel(place_body, shape((tp, rows, LANES), BF16), at, tokens, scalars=1)
    blocks, part_value, part_gate, x = kernel(
        project_body,
        (
            shape((NEAR, 2 * rows + 8, LANES), BF16),
            shape((rows, width), F32),
            shape((rows, width), F32),
            shape((rows, LANES), F32),
        ),
        exchange(placed, "tp"),
        attn_gain.reshape(1, LANES),
        w_query,
        w_key,
        w_value,
        w_gate,
    )
    got = wide_sum(exchange(blocks, "kv", groups_near()))
    vector = got[2 * rows] + got[2 * rows + 1]
    high = lax.reduce_precision(vector, 8, 7)
    tail = jnp.pad(jnp.stack([high, vector - high]), ((0, 6), (0, 0)))
    got = jnp.concatenate([got[: 2 * rows], tail], axis=0)
    got = wide_sum(spread(got.astype(BF16), "kv", far, groups_far()))
    squares = (got[2 * rows] + got[2 * rows + 1])[:rows]
    whole = spread(got[: 2 * rows].astype(BF16), "kv", NEAR, groups_near())
    q_raw, k_raw = side(whole[:, :rows]).astype(F32), side(whole[:, rows:]).astype(F32)

    factor = lax.rsqrt(squares / D + RMS_EPS)[:, None]
    positions = lengths.astype(F32)
    half = DK // 2
    inverse = ROPE_BASE ** (-jnp.arange(half, dtype=F32) / half)
    angles = positions[:, None] * inverse[None, :]
    cosine, sine = jnp.cos(angles), jnp.sin(angles)
    queries = rotate(q_raw * factor, cosine, sine) * DK ** (-0.5)
    keys = rotate(k_raw * factor, cosine, sine)
    by_head = (rows, heads_here, DK)
    own_dot = jnp.sum((queries * keys).reshape(by_head), axis=-1, keepdims=True)
    cached = cache_partial(
        queries.astype(BF16).reshape(by_head),
        lengths,
        log_decay,
        key_cache,
        value_cache,
        heads_here,
    )
    totals = cached + own_dot * (part_value * factor).reshape(by_head)
    totals = totals - jnp.mean(totals, axis=-1, keepdims=True)
    totals = totals.reshape(rows, width)
    gates = part_gate * factor
    both = jnp.stack(
        [
            jnp.concatenate([a[:, n * LANES : (n + 1) * LANES] for a in (totals, gates)], axis=0)
            for n in range(NEAR)
        ]
    )
    got = wide_sum(exchange(both.astype(BF16), "kv", groups_near()))
    got = wide_sum(spread(got.astype(BF16), "kv", far, groups_far()))
    whole = spread(got.astype(BF16), "kv", NEAR, groups_near())

    mixed = kernel(
        mix_body, shape((tp, rows, LANES), BF16), whole, gn_gain.reshape(1, width), w_out
    )
    wide = w_ffn_gate.shape[1]
    cuts = wide // LANES
    packed = -(-(2 * cuts * own + 1) // 8) * 8
    blocks, resid = kernel(
        ffn_in_body,
        (shape((NEAR, packed, LANES), BF16), shape((rows, LANES), BF16)),
        x,
        exchange(mixed, "tp"),
        ffn_gain.reshape(1, LANES),
        w_ffn_gate,
        w_ffn_up,
        scratch=(
            pltpu.VMEM((rows, wide), F32),
            pltpu.VMEM((rows, wide), F32),
            pltpu.VMEM((NEAR, packed, LANES), F32),
        ),
    )
    got = wide_sum(exchange(blocks, "kv", groups_near()))
    arrived = spread(got.astype(BF16), "kv", far, groups_far())
    padded = -(-cuts * own // 8) * 8
    hidden = kernel(
        lambda *refs: hidden_body(*refs, own=own, cuts=cuts),
        shape((NEAR, padded, LANES), BF16),
        arrived,
        scratch=(pltpu.VMEM((packed, LANES), F32),),
    )
    down = kernel(
        down_body,
        shape((tp, rows, LANES), BF16),
        exchange(hidden, "kv", groups_near()),
        w_ffn_down,
        scratch=(pltpu.VMEM((NEAR, padded, LANES), F32), pltpu.VMEM((rows, wide), F32)),
    )
    return kernel(
        last_body, shape(tokens.shape, BF16), at, exchange(down, "tp"), resid, scalars=1
    )


def solution(mesh):
    return jax.shard_map(
        local,
        mesh=mesh,
        in_specs=(
            P("grp", ("kv", "tp")),
            P("grp"),
            P("kv"),
            P("kv", "tp"),
            P("kv", "tp"),
            P("kv", "tp"),
            P("kv", "tp"),
            P("tp"),
            P("grp", "kv", "tp"),
            P("grp", "kv", "tp"),
            P("tp"),
            P("tp", "kv"),
            P("kv"),
            P("kv", "tp"),
            P("kv", "tp"),
            P("tp", "kv"),
        ),
        out_specs=P("grp", ("kv", "tp")),
        check_vma=False,
    )
```

```python
import jax
import jax.numpy as jnp
import numpy as np
from jax import lax
from jax.sharding import PartitionSpec as P

DK = 256
D = 4096
LANES = 128
NEAR = 4

RMS_EPS = 0.1
GN_EPS = 1.0
ROPE_BASE = 10000.0


def groups_near():
    n = lax.axis_size("kv")
    return [list(range(i, i + NEAR)) for i in range(0, n, NEAR)]


def groups_far():
    n = lax.axis_size("kv")
    return [list(range(i, n, NEAR)) for i in range(NEAR)]


def exchange(blocks, axis, groups=None):
    return lax.all_to_all(
        blocks, axis, split_axis=0, concat_axis=0, tiled=True, axis_index_groups=groups
    )


def spread(array, axis, peers, groups=None):
    return exchange(jnp.broadcast_to(array, (peers, *array.shape)), axis, groups)


def wide_sum(blocks):
    return jnp.sum(blocks.astype(jnp.float32), axis=0)


def hi_lo_rows(vector):
    high = lax.reduce_precision(vector, 8, 7)
    rows = jnp.stack([high, vector - high])
    return jnp.pad(rows, ((0, 6), (0, LANES - vector.shape[0])))


def near_blocks(array):
    return jnp.stack(
        [array[:, i * LANES : (i + 1) * LANES] for i in range(array.shape[1] // LANES)]
    )


def side(blocks):
    return jnp.concatenate([blocks[i] for i in range(blocks.shape[0])], axis=1)


def reduce_pair(first, second, extra=None, work=None, inputs=()):
    far = lax.axis_size("kv") // NEAR
    rows = first.shape[0]
    blocks = jnp.concatenate([near_blocks(first), near_blocks(second)], axis=1)
    if extra is not None:
        tail = jnp.broadcast_to(hi_lo_rows(extra), (NEAR, 8, LANES))
        blocks = jnp.concatenate([blocks, tail], axis=1)
    got = wide_sum(exchange(blocks.astype(jnp.bfloat16), "kv", groups_near()))
    if extra is not None:
        vector = got[2 * rows] + got[2 * rows + 1]
        got = jnp.concatenate([got[: 2 * rows], hi_lo_rows(vector[: extra.shape[0]])], axis=0)
    got = got.astype(jnp.bfloat16)
    if work is not None:
        got, inputs = lax.optimization_barrier((got, inputs))
        done = work(*inputs)
    got = spread(got, "kv", far, groups_far())
    if work is not None:
        got, done = lax.optimization_barrier((got, done))
    got = wide_sum(got)
    mine = got[: 2 * rows].astype(jnp.bfloat16)
    if extra is not None:
        vector = (got[2 * rows] + got[2 * rows + 1])[: extra.shape[0]]
        vector = lax.rsqrt(vector / D + RMS_EPS)
        mine, vector = lax.optimization_barrier((mine, vector))
    whole = spread(mine, "kv", NEAR, groups_near())
    outs = (
        side(whole[:, :rows]).astype(jnp.float32),
        side(whole[:, rows:]).astype(jnp.float32),
    )
    if extra is None:
        return outs
    return (*outs, vector, done)


def near_columns(gate, up, stat, padded):
    quarter = gate.shape[1] // NEAR
    rest = padded - quarter
    zeros = jnp.zeros((gate.shape[0], rest), gate.dtype)
    fill = jnp.concatenate([stat[:, None].astype(gate.dtype), zeros[:, 1:]], axis=1)
    blocks = []
    for n in range(NEAR):
        own = slice(n * quarter, (n + 1) * quarter)
        blocks.append(jnp.concatenate([gate[:, own], fill, up[:, own], zeros], axis=1))
    return jnp.stack(blocks)


def rotate(vectors, cosine, sine):
    half = DK // 2
    outs = []
    for h in range(vectors.shape[1] // DK):
        a = vectors[:, h * DK : h * DK + half]
        b = vectors[:, h * DK + half : (h + 1) * DK]
        outs += [a * cosine - b * sine, a * sine + b * cosine]
    return jnp.concatenate(outs, axis=1)


def decay_factors(lengths, log_decay, span, at):
    slots = at * span + jnp.arange(span, dtype=jnp.int32)
    gaps = (lengths[:, None] - slots[None, :]).astype(jnp.float32)
    live = gaps > 0.0
    decays = jnp.exp(log_decay[None, None, :] * jnp.maximum(gaps, 0.0)[:, :, None])
    return jnp.where(live[:, :, None], decays, 0.0)


def cache_partial(query_low, decays, key_cache, value_cache, heads_here):
    batch_rows, span = decays.shape[:2]
    keys_here = key_cache.reshape(batch_rows, span, heads_here, DK)
    values_here = value_cache.reshape(batch_rows, span, heads_here, DK)
    scores = jnp.einsum("bphd,bhd->bph", keys_here, query_low, preferred_element_type=jnp.float32)
    mixing = (scores * decays).astype(jnp.bfloat16)
    return jnp.einsum("bph,bphd->bhd", mixing, values_here, preferred_element_type=jnp.float32)


def local(
    tokens,
    lengths,
    attn_gain,
    w_query,
    w_key,
    w_value,
    w_gate,
    log_decay,
    key_cache,
    value_cache,
    gn_gain,
    w_out,
    ffn_gain,
    w_ffn_gate,
    w_ffn_up,
    w_ffn_down,
):
    rows = tokens.shape[0]
    heads_here = log_decay.shape[0]
    kv = lax.axis_size("kv")
    tp = lax.axis_size("tp")
    own_width = tokens.shape[1]
    gathered = spread(tokens, "tp", tp)
    x = jnp.moveaxis(gathered, 0, 1).reshape(rows, tp * own_width).astype(jnp.float32)
    own_squares = jnp.sum(x * x, axis=1)
    scaled = (x * attn_gain).astype(jnp.bfloat16)
    dot = lambda a, w: jnp.dot(a, w, preferred_element_type=jnp.float32)

    def ahead(scaled, lengths, log_decay, w_value, w_gate, kv_at):
        half = DK // 2
        inverse = (ROPE_BASE ** (-np.arange(half) / half)).astype(np.float32)
        angles = lengths.astype(jnp.float32)[:, None] * inverse[None, :]
        return (
            jnp.cos(angles),
            jnp.sin(angles),
            decay_factors(lengths, log_decay, key_cache.shape[1], kv_at),
            dot(scaled, w_value),
            dot(scaled, w_gate),
        )

    q_raw, k_raw, factor, made = reduce_pair(
        dot(scaled, w_query),
        dot(scaled, w_key),
        own_squares,
        ahead,
        (scaled, lengths, log_decay, w_value, w_gate, lax.axis_index("kv")),
    )
    cosine, sine, decays, part_value, part_gate = made
    factor = factor[:, None]
    queries = rotate(q_raw * factor, cosine, sine) * DK ** (-0.5)
    keys = rotate(k_raw * factor, cosine, sine)
    by_head = (rows, heads_here, DK)
    own_dot = jnp.sum((queries * keys).reshape(by_head), axis=-1, keepdims=True)
    cached = cache_partial(
        queries.astype(jnp.bfloat16).reshape(by_head),
        decays,
        key_cache,
        value_cache,
        heads_here,
    )
    part_value = part_value * factor
    totals = cached + own_dot * part_value.reshape(by_head)
    totals = totals - jnp.mean(totals, axis=-1, keepdims=True)
    part_gate = part_gate * factor
    totals, gates = reduce_pair(totals.reshape(rows, heads_here * DK), part_gate)
    totals = totals.reshape(by_head)
    center = jnp.mean(totals, axis=-1, keepdims=True)
    spread_ = jnp.mean(totals * totals, axis=-1, keepdims=True) - center * center
    normed = ((totals - center) * lax.rsqrt(spread_ + GN_EPS)).reshape(rows, heads_here * DK)
    gated = (jax.nn.silu(gates) * (normed * gn_gain)).astype(jnp.bfloat16)
    mixed = dot(gated, w_out).astype(jnp.bfloat16)
    own_at = (lax.axis_index("tp") * own_width).astype(jnp.uint32)
    mixed, own_at = lax.optimization_barrier((mixed, own_at))
    mixed = wide_sum(spread(mixed, "tp", tp))
    resid = (x + mixed).astype(jnp.bfloat16)
    resid_wide = resid.astype(jnp.float32)
    mid_squares = jnp.sum(resid_wide * resid_wide, axis=1)
    scaled_mid = (resid_wide * ffn_gain).astype(jnp.bfloat16)
    own_resid = lax.dynamic_slice(resid_wide, (jnp.uint32(0), own_at), (rows, own_width))
    quarter = w_ffn_gate.shape[1] // NEAR
    padded = -(-(quarter + 1) // LANES) * LANES
    blocks = near_columns(
        dot(scaled_mid, w_ffn_gate).astype(jnp.bfloat16),
        dot(scaled_mid, w_ffn_up).astype(jnp.bfloat16),
        mid_squares,
        padded,
    )
    blocks, own_resid = lax.optimization_barrier((blocks, own_resid))
    got = wide_sum(exchange(blocks, "kv", groups_near()))
    got = wide_sum(spread(got.astype(jnp.bfloat16), "kv", kv // NEAR, groups_far()))
    factor_mid = lax.rsqrt(got[:, quarter : quarter + 1] / D + RMS_EPS)
    hidden = jax.nn.silu(got[:, :padded] * factor_mid) * (got[:, padded:] * factor_mid)
    whole = spread(hidden.astype(jnp.bfloat16), "kv", NEAR, groups_near())
    hidden = side(whole[:, :, :quarter])
    down_part = dot(hidden, w_ffn_down).astype(jnp.bfloat16)
    down = wide_sum(
        exchange(jnp.moveaxis(down_part.reshape(rows, tp, own_width), 1, 0), "tp")
    )
    return (own_resid + down).astype(jnp.bfloat16)


def solution(mesh):
    return jax.shard_map(
        local,
        mesh=mesh,
        in_specs=(
            P("grp", ("kv", "tp")),
            P("grp"),
            P("kv"),
            P("kv", "tp"),
            P("kv", "tp"),
            P("kv", "tp"),
            P("kv", "tp"),
            P("tp"),
            P("grp", "kv", "tp"),
            P("grp", "kv", "tp"),
            P("tp"),
            P("tp", "kv"),
            P("kv"),
            P("kv", "tp"),
            P("kv", "tp"),
            P("tp", "kv"),
        ),
        out_specs=P("grp", ("kv", "tp")),
        check_vma=False,
    )
```

```python
import jax
import jax.numpy as jnp
import numpy as np
from jax import lax
from jax.sharding import PartitionSpec as P

DK = 256
D = 4096
LANES = 128
NEAR = 4

RMS_EPS = 0.1
GN_EPS = 1.0
ROPE_BASE = 10000.0


def groups_near():
    n = lax.axis_size("kv")
    return [list(range(i, i + NEAR)) for i in range(0, n, NEAR)]


def groups_far():
    n = lax.axis_size("kv")
    return [list(range(i, n, NEAR)) for i in range(NEAR)]


def exchange(blocks, axis, groups=None):
    return lax.all_to_all(
        blocks, axis, split_axis=0, concat_axis=0, tiled=True, axis_index_groups=groups
    )


def spread(array, axis, peers, groups=None):
    return exchange(jnp.broadcast_to(array, (peers, *array.shape)), axis, groups)


def wide_sum(blocks):
    return jnp.sum(blocks.astype(jnp.float32), axis=0)


def hi_lo_rows(vector):
    high = lax.reduce_precision(vector, 8, 7)
    rows = jnp.stack([high, vector - high])
    return jnp.pad(rows, ((0, 6), (0, LANES - vector.shape[0])))


def near_blocks(array):
    return jnp.stack(
        [array[:, i * LANES : (i + 1) * LANES] for i in range(array.shape[1] // LANES)]
    )


def side(blocks):
    return jnp.concatenate([blocks[i] for i in range(blocks.shape[0])], axis=1)


def reduce_pair(first, second, extra=None, work=None, inputs=()):
    far = lax.axis_size("kv") // NEAR
    rows = first.shape[0]
    blocks = jnp.concatenate([near_blocks(first), near_blocks(second)], axis=1)
    if extra is not None:
        tail = jnp.broadcast_to(hi_lo_rows(extra), (NEAR, 8, LANES))
        blocks = jnp.concatenate([blocks, tail], axis=1)
    got = wide_sum(exchange(blocks.astype(jnp.bfloat16), "kv", groups_near()))
    if extra is not None:
        vector = got[2 * rows] + got[2 * rows + 1]
        got = jnp.concatenate([got[: 2 * rows], hi_lo_rows(vector[: extra.shape[0]])], axis=0)
    got = got.astype(jnp.bfloat16)
    if work is not None:
        got, inputs = lax.optimization_barrier((got, inputs))
        done = work(*inputs)
    got = spread(got, "kv", far, groups_far())
    if work is not None:
        got, done = lax.optimization_barrier((got, done))
    got = wide_sum(got)
    mine = got[: 2 * rows].astype(jnp.bfloat16)
    if extra is not None:
        vector = (got[2 * rows] + got[2 * rows + 1])[: extra.shape[0]]
        vector = lax.rsqrt(vector / D + RMS_EPS)
        mine, vector = lax.optimization_barrier((mine, vector))
    whole = spread(mine, "kv", NEAR, groups_near())
    outs = (
        side(whole[:, :rows]).astype(jnp.float32),
        side(whole[:, rows:]).astype(jnp.float32),
    )
    if extra is None:
        return outs
    return (*outs, vector, done)


def near_columns(gate, up, stat, padded):
    quarter = gate.shape[1] // NEAR
    rest = padded - quarter
    zeros = jnp.zeros((gate.shape[0], rest), gate.dtype)
    fill = jnp.concatenate([stat[:, None].astype(gate.dtype), zeros[:, 1:]], axis=1)
    blocks = []
    for n in range(NEAR):
        own = slice(n * quarter, (n + 1) * quarter)
        blocks.append(jnp.concatenate([gate[:, own], fill, up[:, own], zeros], axis=1))
    return jnp.stack(blocks)


def rotate(vectors, cosine, sine):
    half = DK // 2
    outs = []
    for h in range(vectors.shape[1] // DK):
        a = vectors[:, h * DK : h * DK + half]
        b = vectors[:, h * DK + half : (h + 1) * DK]
        outs += [a * cosine - b * sine, a * sine + b * cosine]
    return jnp.concatenate(outs, axis=1)


def decay_factors(lengths, log_decay, span, at):
    slots = at * span + jnp.arange(span, dtype=jnp.int32)
    gaps = (lengths[:, None] - slots[None, :]).astype(jnp.float32)
    live = gaps > 0.0
    decays = jnp.exp(log_decay[None, None, :] * jnp.maximum(gaps, 0.0)[:, :, None])
    return jnp.where(live[:, :, None], decays, 0.0)


def cache_partial(query_low, decays, key_cache, value_cache, heads_here):
    batch_rows, span = decays.shape[:2]
    keys_here = key_cache.reshape(batch_rows, span, heads_here, DK)
    values_here = value_cache.reshape(batch_rows, span, heads_here, DK)
    scores = jnp.einsum("bphd,bhd->bph", keys_here, query_low, preferred_element_type=jnp.float32)
    mixing = (scores * decays).astype(jnp.bfloat16)
    return jnp.einsum("bph,bphd->bhd", mixing, values_here, preferred_element_type=jnp.float32)


def local(
    tokens,
    lengths,
    attn_gain,
    w_query,
    w_key,
    w_value,
    w_gate,
    log_decay,
    key_cache,
    value_cache,
    gn_gain,
    w_out,
    ffn_gain,
    w_ffn_gate,
    w_ffn_up,
    w_ffn_down,
):
    rows = tokens.shape[0]
    heads_here = log_decay.shape[0]
    tp = lax.axis_size("tp")
    own_width = tokens.shape[1]
    kv_at = lax.axis_index("kv")
    own_at = (lax.axis_index("tp") * own_width).astype(jnp.uint32)
    tokens, kv_at, own_at = lax.optimization_barrier((tokens, kv_at, own_at))
    gathered = spread(tokens, "tp", tp)
    x = jnp.moveaxis(gathered, 0, 1).reshape(rows, tp * own_width).astype(jnp.float32)
    own_squares = jnp.sum(x * x, axis=1)
    scaled = (x * attn_gain).astype(jnp.bfloat16)
    dot = lambda a, w: jnp.dot(a, w, preferred_element_type=jnp.float32)

    def ahead(scaled, lengths, log_decay, w_value, w_gate, kv_at):
        half = DK // 2
        inverse = (ROPE_BASE ** (-np.arange(half) / half)).astype(np.float32)
        angles = lengths.astype(jnp.float32)[:, None] * inverse[None, :]
        return (
            jnp.cos(angles),
            jnp.sin(angles),
            decay_factors(lengths, log_decay, key_cache.shape[1], kv_at),
            dot(scaled, w_value),
            dot(scaled, w_gate),
        )

    q_raw, k_raw, factor, made = reduce_pair(
        dot(scaled, w_query),
        dot(scaled, w_key),
        own_squares,
        ahead,
        (scaled, lengths, log_decay, w_value, w_gate, kv_at),
    )
    cosine, sine, decays, part_value, part_gate = made
    factor = factor[:, None]
    queries = rotate(q_raw * factor, cosine, sine) * DK ** (-0.5)
    keys = rotate(k_raw * factor, cosine, sine)
    by_head = (rows, heads_here, DK)
    own_dot = jnp.sum((queries * keys).reshape(by_head), axis=-1, keepdims=True)
    cached = cache_partial(
        queries.astype(jnp.bfloat16).reshape(by_head),
        decays,
        key_cache,
        value_cache,
        heads_here,
    )
    part_value = part_value * factor
    totals = cached + own_dot * part_value.reshape(by_head)
    totals = totals - jnp.mean(totals, axis=-1, keepdims=True)
    part_gate = part_gate * factor
    totals, gates = reduce_pair(totals.reshape(rows, heads_here * DK), part_gate)
    totals = totals.reshape(by_head)
    center = jnp.mean(totals, axis=-1, keepdims=True)
    spread_ = jnp.mean(totals * totals, axis=-1, keepdims=True) - center * center
    normed = ((totals - center) * lax.rsqrt(spread_ + GN_EPS)).reshape(rows, heads_here * DK)
    gated = (jax.nn.silu(gates) * (normed * gn_gain)).astype(jnp.bfloat16)
    mixed = dot(gated, w_out).astype(jnp.bfloat16)
    mixed = wide_sum(spread(mixed, "tp", tp))
    resid = (x + mixed).astype(jnp.bfloat16)
    resid_wide = resid.astype(jnp.float32)
    mid_squares = jnp.sum(resid_wide * resid_wide, axis=1)
    scaled_mid = (resid_wide * ffn_gain).astype(jnp.bfloat16)
    own_resid = lax.dynamic_slice(resid_wide, (jnp.uint32(0), own_at), (rows, own_width))
    quarter = w_ffn_gate.shape[1] // NEAR
    padded = -(-(quarter + 1) // LANES) * LANES
    blocks = near_columns(
        dot(scaled_mid, w_ffn_gate).astype(jnp.bfloat16),
        dot(scaled_mid, w_ffn_up).astype(jnp.bfloat16),
        mid_squares,
        padded,
    )
    blocks, own_resid = lax.optimization_barrier((blocks, own_resid))
    got = wide_sum(exchange(blocks, "kv", groups_near()))
    got = wide_sum(
        lax.all_gather(got.astype(jnp.bfloat16), "kv", axis_index_groups=groups_far())
    )
    factor_mid = lax.rsqrt(got[:, quarter : quarter + 1] / D + RMS_EPS)
    hidden = jax.nn.silu(got[:, :padded] * factor_mid) * (got[:, padded:] * factor_mid)
    whole = spread(hidden.astype(jnp.bfloat16), "kv", NEAR, groups_near())
    hidden = side(whole[:, :, :quarter])
    down_part = dot(hidden, w_ffn_down).astype(jnp.bfloat16)
    down = wide_sum(
        exchange(jnp.moveaxis(down_part.reshape(rows, tp, own_width), 1, 0), "tp")
    )
    return (own_resid + down).astype(jnp.bfloat16)


def solution(mesh):
    return jax.shard_map(
        local,
        mesh=mesh,
        in_specs=(
            P("grp", ("kv", "tp")),
            P("grp"),
            P("kv"),
            P("kv", "tp"),
            P("kv", "tp"),
            P("kv", "tp"),
            P("kv", "tp"),
            P("tp"),
            P("grp", "kv", "tp"),
            P("grp", "kv", "tp"),
            P("tp"),
            P("tp", "kv"),
            P("kv"),
            P("kv", "tp"),
            P("kv", "tp"),
            P("tp", "kv"),
        ),
        out_specs=P("grp", ("kv", "tp")),
        check_vma=False,
    )
```

```python
import jax
import jax.numpy as jnp
import numpy as np
from jax import lax
from jax.sharding import PartitionSpec as P

DK = 256
D = 4096
LANES = 128
NEAR = 4

RMS_EPS = 0.1
GN_EPS = 1.0
ROPE_BASE = 10000.0


def groups_near():
    n = lax.axis_size("kv")
    return [list(range(i, i + NEAR)) for i in range(0, n, NEAR)]


def groups_far():
    n = lax.axis_size("kv")
    return [list(range(i, n, NEAR)) for i in range(NEAR)]


def exchange(blocks, axis, groups=None):
    return lax.all_to_all(
        blocks, axis, split_axis=0, concat_axis=0, tiled=True, axis_index_groups=groups
    )


def spread(array, axis, peers, groups=None):
    return exchange(jnp.broadcast_to(array, (peers, *array.shape)), axis, groups)


def wide_sum(blocks):
    return jnp.sum(blocks.astype(jnp.float32), axis=0)


def hi_lo_rows(vector):
    high = lax.reduce_precision(vector, 8, 7)
    rows = jnp.stack([high, vector - high])
    return jnp.pad(rows, ((0, 6), (0, LANES - vector.shape[0])))


def near_blocks(array):
    return jnp.stack(
        [array[:, i * LANES : (i + 1) * LANES] for i in range(array.shape[1] // LANES)]
    )


def side(blocks):
    return jnp.concatenate([blocks[i] for i in range(blocks.shape[0])], axis=1)


def reduce_pair(first, second, extra=None, work=None, inputs=()):
    far = lax.axis_size("kv") // NEAR
    rows = first.shape[0]
    blocks = jnp.concatenate([near_blocks(first), near_blocks(second)], axis=1)
    if extra is not None:
        tail = jnp.broadcast_to(hi_lo_rows(extra), (NEAR, 8, LANES))
        blocks = jnp.concatenate([blocks, tail], axis=1)
    blocks, inputs = lax.optimization_barrier((blocks.astype(jnp.bfloat16), inputs))
    got = wide_sum(exchange(blocks, "kv", groups_near()))
    if extra is not None:
        vector = got[2 * rows] + got[2 * rows + 1]
        got = jnp.concatenate([got[: 2 * rows], hi_lo_rows(vector[: extra.shape[0]])], axis=0)
    got = got.astype(jnp.bfloat16)
    if work is not None:
        got, inputs = lax.optimization_barrier((got, inputs))
        done = work(*inputs)
    got = spread(got, "kv", far, groups_far())
    if work is not None:
        got, done = lax.optimization_barrier((got, done))
    got = wide_sum(got)
    mine = got[: 2 * rows].astype(jnp.bfloat16)
    if extra is not None:
        vector = (got[2 * rows] + got[2 * rows + 1])[: extra.shape[0]]
        vector = lax.rsqrt(vector / D + RMS_EPS)
        mine, vector = lax.optimization_barrier((mine, vector))
    whole = spread(mine, "kv", NEAR, groups_near())
    outs = (
        side(whole[:, :rows]).astype(jnp.float32),
        side(whole[:, rows:]).astype(jnp.float32),
    )
    if extra is None:
        return outs
    return (*outs, vector, done)


def near_columns(gate, up, stat, padded):
    quarter = gate.shape[1] // NEAR
    rest = padded - quarter
    zeros = jnp.zeros((gate.shape[0], rest), gate.dtype)
    fill = jnp.concatenate([stat[:, None].astype(gate.dtype), zeros[:, 1:]], axis=1)
    blocks = []
    for n in range(NEAR):
        own = slice(n * quarter, (n + 1) * quarter)
        blocks.append(jnp.concatenate([gate[:, own], fill, up[:, own], zeros], axis=1))
    return jnp.stack(blocks)


def rotate(vectors, cosine, sine):
    half = DK // 2
    outs = []
    for h in range(vectors.shape[1] // DK):
        a = vectors[:, h * DK : h * DK + half]
        b = vectors[:, h * DK + half : (h + 1) * DK]
        outs += [a * cosine - b * sine, a * sine + b * cosine]
    return jnp.concatenate(outs, axis=1)


def decay_factors(lengths, log_decay, span, at):
    slots = at * span + jnp.arange(span, dtype=jnp.int32)
    gaps = (lengths[:, None] - slots[None, :]).astype(jnp.float32)
    live = gaps > 0.0
    decays = jnp.exp(log_decay[None, None, :] * jnp.maximum(gaps, 0.0)[:, :, None])
    return jnp.where(live[:, :, None], decays, 0.0)


def cache_partial(query_low, decays, key_cache, value_cache, heads_here):
    batch_rows, span = decays.shape[:2]
    keys_here = key_cache.reshape(batch_rows, span, heads_here, DK)
    values_here = value_cache.reshape(batch_rows, span, heads_here, DK)
    scores = jnp.einsum("bphd,bhd->bph", keys_here, query_low, preferred_element_type=jnp.float32)
    mixing = (scores * decays).astype(jnp.bfloat16)
    return jnp.einsum("bph,bphd->bhd", mixing, values_here, preferred_element_type=jnp.float32)


def local(
    tokens,
    lengths,
    attn_gain,
    w_query,
    w_key,
    w_value,
    w_gate,
    log_decay,
    key_cache,
    value_cache,
    gn_gain,
    w_out,
    ffn_gain,
    w_ffn_gate,
    w_ffn_up,
    w_ffn_down,
):
    rows = tokens.shape[0]
    heads_here = log_decay.shape[0]
    tp = lax.axis_size("tp")
    own_width = tokens.shape[1]
    kv_at = lax.axis_index("kv")
    own_at = (lax.axis_index("tp") * own_width).astype(jnp.uint32)
    tokens, kv_at, own_at = lax.optimization_barrier((tokens, kv_at, own_at))
    own_gain = lax.dynamic_slice(attn_gain, (own_at,), (own_width,))
    own_scaled = (tokens.astype(jnp.float32) * own_gain[None, :]).astype(jnp.bfloat16)
    gathered = spread(jnp.stack([tokens, own_scaled]), "tp", tp)
    x, scaled = (
        jnp.moveaxis(gathered[:, i], 0, 1).reshape(rows, tp * own_width) for i in (0, 1)
    )
    own_squares = jnp.sum(x.astype(jnp.float32) * x.astype(jnp.float32), axis=1)
    dot = lambda a, w: jnp.dot(a, w, preferred_element_type=jnp.float32)

    quarter = w_ffn_gate.shape[1] // NEAR
    padded = -(-(quarter + 1) // LANES) * LANES

    def with_gain(gain, w):
        return (gain[:, None] * w.astype(jnp.float32)).astype(jnp.bfloat16)

    def ahead(
        x, scaled, lengths, log_decay, w_value, w_gate, kv_at, gn_gain, w_out, ffn_gain, w_fg, w_fu
    ):
        half = DK // 2
        inverse = (ROPE_BASE ** (-np.arange(half) / half)).astype(np.float32)
        angles = lengths.astype(jnp.float32)[:, None] * inverse[None, :]
        return (
            jnp.cos(angles),
            jnp.sin(angles),
            decay_factors(lengths, log_decay, key_cache.shape[1], kv_at),
            dot(scaled, w_value),
            dot(scaled, w_gate),
            x.astype(jnp.float32),
            with_gain(gn_gain, w_out),
            with_gain(ffn_gain, w_fg),
            with_gain(ffn_gain, w_fu),
        )

    q_raw, k_raw, factor, made = reduce_pair(
        dot(scaled, w_query),
        dot(scaled, w_key),
        own_squares,
        ahead,
        (
            x,
            scaled,
            lengths,
            log_decay,
            w_value,
            w_gate,
            kv_at,
            gn_gain,
            w_out,
            ffn_gain,
            w_ffn_gate,
            w_ffn_up,
        ),
    )
    cosine, sine, decays, part_value, part_gate, x, out_gained, gate_gained, up_gained = made
    factor = factor[:, None]
    queries = rotate(q_raw * factor, cosine, sine) * DK ** (-0.5)
    keys = rotate(k_raw * factor, cosine, sine)
    by_head = (rows, heads_here, DK)
    own_dot = jnp.sum((queries * keys).reshape(by_head), axis=-1, keepdims=True)
    cached = cache_partial(
        queries.astype(jnp.bfloat16).reshape(by_head),
        decays,
        key_cache,
        value_cache,
        heads_here,
    )
    part_value = part_value * factor
    totals = cached + own_dot * part_value.reshape(by_head)
    totals = totals - jnp.mean(totals, axis=-1, keepdims=True)
    part_gate = part_gate * factor
    totals, gates = reduce_pair(totals.reshape(rows, heads_here * DK), part_gate)
    totals = totals.reshape(by_head)
    center = jnp.mean(totals, axis=-1, keepdims=True)
    spread_ = jnp.mean(totals * totals, axis=-1, keepdims=True) - center * center
    normed = ((totals - center) * lax.rsqrt(spread_ + GN_EPS)).reshape(rows, heads_here * DK)
    gated = (jax.nn.silu(gates) * normed).astype(jnp.bfloat16)
    mixed = dot(gated, out_gained).astype(jnp.bfloat16)
    mixed = wide_sum(spread(mixed, "tp", tp))
    resid = (x + mixed).astype(jnp.bfloat16)
    resid_wide = resid.astype(jnp.float32)
    mid_squares = jnp.sum(resid_wide * resid_wide, axis=1)
    own_resid = lax.dynamic_slice(resid_wide, (jnp.uint32(0), own_at), (rows, own_width))
    blocks = near_columns(
        dot(resid, gate_gained).astype(jnp.bfloat16),
        dot(resid, up_gained).astype(jnp.bfloat16),
        mid_squares,
        padded,
    )
    blocks, own_resid = lax.optimization_barrier((blocks, own_resid))
    got = wide_sum(exchange(blocks, "kv", groups_near()))
    got = wide_sum(
        lax.all_gather(got.astype(jnp.bfloat16), "kv", axis_index_groups=groups_far())
    )
    factor_mid = lax.rsqrt(got[:, quarter : quarter + 1] / D + RMS_EPS)
    hidden = jax.nn.silu(got[:, :padded] * factor_mid) * (got[:, padded:] * factor_mid)
    whole = spread(hidden.astype(jnp.bfloat16), "kv", NEAR, groups_near())
    hidden = side(whole[:, :, :quarter])
    down_part = dot(hidden, w_ffn_down).astype(jnp.bfloat16)
    down = wide_sum(
        exchange(jnp.moveaxis(down_part.reshape(rows, tp, own_width), 1, 0), "tp")
    )
    return (own_resid + down).astype(jnp.bfloat16)


def solution(mesh):
    return jax.shard_map(
        local,
        mesh=mesh,
        in_specs=(
            P("grp", ("kv", "tp")),
            P("grp"),
            P("kv"),
            P("kv", "tp"),
            P("kv", "tp"),
            P("kv", "tp"),
            P("kv", "tp"),
            P("tp"),
            P("grp", "kv", "tp"),
            P("grp", "kv", "tp"),
            P("tp"),
            P("tp", "kv"),
            P("kv"),
            P("kv", "tp"),
            P("kv", "tp"),
            P("tp", "kv"),
        ),
        out_specs=P("grp", ("kv", "tp")),
        check_vma=False,
    )
```

```python
import jax
import jax.numpy as jnp
import numpy as np
from jax import lax
from jax.sharding import PartitionSpec as P

DK = 256
D = 4096
LANES = 128
NEAR = 4

RMS_EPS = 0.1
GN_EPS = 1.0
ROPE_BASE = 10000.0


def groups_near():
    n = lax.axis_size("kv")
    return [list(range(i, i + NEAR)) for i in range(0, n, NEAR)]


def groups_far():
    n = lax.axis_size("kv")
    return [list(range(i, n, NEAR)) for i in range(NEAR)]


def exchange(blocks, axis, groups=None):
    return lax.all_to_all(
        blocks, axis, split_axis=0, concat_axis=0, tiled=True, axis_index_groups=groups
    )


def spread(array, axis, peers, groups=None):
    return exchange(jnp.broadcast_to(array, (peers, *array.shape)), axis, groups)


def wide_sum(blocks):
    return jnp.sum(blocks.astype(jnp.float32), axis=0)


def hi_lo_rows(vector):
    high = lax.reduce_precision(vector, 8, 7)
    rows = jnp.stack([high, vector - high])
    return jnp.pad(rows, ((0, 6), (0, LANES - vector.shape[0])))


def near_blocks(array):
    return jnp.stack(
        [array[:, i * LANES : (i + 1) * LANES] for i in range(array.shape[1] // LANES)]
    )


def side(blocks):
    return jnp.concatenate([blocks[i] for i in range(blocks.shape[0])], axis=1)


def reduce_pair(first, second, extra=None, work=None, inputs=()):
    far = lax.axis_size("kv") // NEAR
    rows = first.shape[1]
    blocks = jnp.concatenate([first, second], axis=1)
    if extra is not None:
        tail = jnp.broadcast_to(hi_lo_rows(extra), (NEAR, 8, LANES))
        blocks = jnp.concatenate([blocks, tail], axis=1)
    blocks, inputs = lax.optimization_barrier((blocks.astype(jnp.bfloat16), inputs))
    got = wide_sum(exchange(blocks, "kv", groups_near()))
    if extra is not None:
        vector = got[2 * rows] + got[2 * rows + 1]
        got = jnp.concatenate([got[: 2 * rows], hi_lo_rows(vector[: extra.shape[0]])], axis=0)
    got = got.astype(jnp.bfloat16)
    if work is not None:
        got, inputs = lax.optimization_barrier((got, inputs))
        done = work(*inputs)
    got = spread(got, "kv", far, groups_far())
    if work is not None:
        got, done = lax.optimization_barrier((got, done))
    got = wide_sum(got)
    mine = got[: 2 * rows].astype(jnp.bfloat16)
    if extra is not None:
        vector = (got[2 * rows] + got[2 * rows + 1])[: extra.shape[0]]
        vector = lax.rsqrt(vector / D + RMS_EPS)
        mine, vector = lax.optimization_barrier((mine, vector))
    whole = spread(mine, "kv", NEAR, groups_near())
    if extra is not None:
        whole, vector = lax.optimization_barrier((whole, vector))
    outs = (whole[:, :rows].astype(jnp.float32), whole[:, rows:].astype(jnp.float32))
    if extra is None:
        return outs
    return (*outs, vector, done)


def near_columns(gate, up, stat, padded):
    quarter = gate.shape[1] // NEAR
    rest = padded - quarter
    zeros = jnp.zeros((gate.shape[0], rest), gate.dtype)
    fill = jnp.concatenate([stat[:, None].astype(gate.dtype), zeros[:, 1:]], axis=1)
    blocks = []
    for n in range(NEAR):
        own = slice(n * quarter, (n + 1) * quarter)
        blocks.append(jnp.concatenate([gate[:, own], fill, up[:, own], zeros], axis=1))
    return jnp.stack(blocks)


def rotate(halves, cosine, sine):
    outs = []
    for h in range(0, halves.shape[0], 2):
        a, b = halves[h], halves[h + 1]
        outs += [a * cosine - b * sine, a * sine + b * cosine]
    return outs


def decay_factors(lengths, log_decay, span, at):
    slots = at * span + jnp.arange(span, dtype=jnp.int32)
    gaps = (lengths[:, None] - slots[None, :]).astype(jnp.float32)
    live = gaps > 0.0
    decays = jnp.exp(log_decay[None, :, None] * jnp.maximum(gaps, 0.0)[:, None, :])
    return jnp.where(live[:, None, :], decays, 0.0)


def cache_partial(query_low, decays, key_cache, value_cache, heads_here):
    batch_rows, _, span = decays.shape
    keys_here = key_cache.reshape(batch_rows, span, heads_here, DK)
    values_here = value_cache.reshape(batch_rows, span, heads_here, DK)
    scores = jnp.einsum("bphd,bhd->bhp", keys_here, query_low, preferred_element_type=jnp.float32)
    mixing = (scores * decays).astype(jnp.bfloat16)
    return jnp.einsum("bhp,bphd->bhd", mixing, values_here, preferred_element_type=jnp.float32)


def local(
    tokens,
    lengths,
    attn_gain,
    w_query,
    w_key,
    w_value,
    w_gate,
    log_decay,
    key_cache,
    value_cache,
    gn_gain,
    w_out,
    ffn_gain,
    w_ffn_gate,
    w_ffn_up,
    w_ffn_down,
):
    rows = tokens.shape[0]
    heads_here = log_decay.shape[0]
    tp = lax.axis_size("tp")
    own_width = tokens.shape[1]
    kv_at = lax.axis_index("kv")
    own_at = (lax.axis_index("tp") * own_width).astype(jnp.uint32)
    tokens, kv_at, own_at = lax.optimization_barrier((tokens, kv_at, own_at))
    own_gain = lax.dynamic_slice(attn_gain, (own_at,), (own_width,))
    own_scaled = (tokens.astype(jnp.float32) * own_gain[None, :]).astype(jnp.bfloat16)
    gathered = spread(jnp.stack([tokens, own_scaled]), "tp", tp)
    x, scaled = (
        jnp.moveaxis(gathered[:, i], 0, 1).reshape(rows, tp * own_width) for i in (0, 1)
    )
    own_squares = jnp.sum(x.astype(jnp.float32) * x.astype(jnp.float32), axis=1)
    dot = lambda a, w: jnp.dot(a, w, preferred_element_type=jnp.float32)

    quarter = w_ffn_gate.shape[1] // NEAR
    padded = -(-(quarter + 1) // LANES) * LANES

    def with_gain(gain, w):
        return (gain[:, None] * w.astype(jnp.float32)).astype(jnp.bfloat16)

    def ahead(
        x, scaled, lengths, log_decay, w_value, w_gate, kv_at, gn_gain, w_out, ffn_gain, w_fg, w_fu
    ):
        half = DK // 2
        inverse = (ROPE_BASE ** (-np.arange(half) / half)).astype(np.float32)
        angles = lengths.astype(jnp.float32)[:, None] * inverse[None, :]
        return (
            jnp.cos(angles),
            jnp.sin(angles),
            decay_factors(lengths, log_decay, key_cache.shape[1], kv_at),
            dot(scaled, w_value),
            dot(scaled, w_gate),
            x.astype(jnp.float32),
            with_gain(gn_gain, w_out),
            with_gain(ffn_gain, w_fg),
            with_gain(ffn_gain, w_fu),
        )

    q_raw, k_raw, factor, made = reduce_pair(
        near_blocks(dot(scaled, w_query)),
        near_blocks(dot(scaled, w_key)),
        own_squares,
        ahead,
        (
            x,
            scaled,
            lengths,
            log_decay,
            w_value,
            w_gate,
            kv_at,
            gn_gain,
            w_out,
            ffn_gain,
            w_ffn_gate,
            w_ffn_up,
        ),
    )
    cosine, sine, decays, part_value, part_gate, x, out_gained, gate_gained, up_gained = made
    factor = factor[:, None]
    queries = [a * DK ** (-0.5) for a in rotate(q_raw * factor, cosine, sine)]
    keys = rotate(k_raw * factor, cosine, sine)
    cached = cache_partial(
        jnp.concatenate(queries, axis=1).astype(jnp.bfloat16).reshape(rows, heads_here, DK),
        decays,
        key_cache,
        value_cache,
        heads_here,
    )
    totals = []
    for h in range(heads_here):
        two = (2 * h, 2 * h + 1)
        own_dot = sum(jnp.sum(queries[n] * keys[n], axis=1, keepdims=True) for n in two)
        value = part_value[:, h * DK : (h + 1) * DK] * factor
        total = cached[:, h] + own_dot * value
        total = total - jnp.mean(total, axis=1, keepdims=True)
        totals += [total[:, :LANES], total[:, LANES:]]
    totals, gates = reduce_pair(jnp.stack(totals), near_blocks(part_gate * factor))
    gated = []
    for h in range(heads_here):
        a, b = totals[2 * h], totals[2 * h + 1]
        center = (jnp.sum(a, axis=1, keepdims=True) + jnp.sum(b, axis=1, keepdims=True)) / DK
        a, b = a - center, b - center
        spread_ = jnp.sum(a * a, axis=1, keepdims=True) + jnp.sum(b * b, axis=1, keepdims=True)
        scale = lax.rsqrt(spread_ / DK + GN_EPS)
        gated += [
            (jax.nn.silu(gates[2 * h]) * (a * scale)).astype(jnp.bfloat16),
            (jax.nn.silu(gates[2 * h + 1]) * (b * scale)).astype(jnp.bfloat16),
        ]
    gated = jnp.concatenate(gated, axis=1)
    mixed = dot(gated, out_gained).astype(jnp.bfloat16)
    mixed = wide_sum(spread(mixed, "tp", tp))
    resid = (x + mixed).astype(jnp.bfloat16)
    resid_wide = resid.astype(jnp.float32)
    mid_squares = jnp.sum(resid_wide * resid_wide, axis=1)
    blocks = near_columns(
        dot(resid, gate_gained).astype(jnp.bfloat16),
        dot(resid, up_gained).astype(jnp.bfloat16),
        mid_squares,
        padded,
    )
    got = wide_sum(exchange(blocks, "kv", groups_near()))
    got = wide_sum(
        lax.all_gather(got.astype(jnp.bfloat16), "kv", axis_index_groups=groups_far())
    )
    factor_mid = lax.rsqrt(got[:, quarter : quarter + 1] / D + RMS_EPS)
    hidden = jax.nn.silu(got[:, :padded] * factor_mid) * (got[:, padded:] * factor_mid)
    whole = spread(hidden.astype(jnp.bfloat16), "kv", NEAR, groups_near())
    hidden = side(whole[:, :, :quarter])
    down_part = dot(hidden, w_ffn_down).astype(jnp.bfloat16)
    down = wide_sum(spread(down_part, "tp", tp))
    return lax.dynamic_slice(
        (resid_wide + down).astype(jnp.bfloat16), (jnp.uint32(0), own_at), (rows, own_width)
    )


def solution(mesh):
    return jax.shard_map(
        local,
        mesh=mesh,
        in_specs=(
            P("grp", ("kv", "tp")),
            P("grp"),
            P("kv"),
            P("kv", "tp"),
            P("kv", "tp"),
            P("kv", "tp"),
            P("kv", "tp"),
            P("tp"),
            P("grp", "kv", "tp"),
            P("grp", "kv", "tp"),
            P("tp"),
            P("tp", "kv"),
            P("kv"),
            P("kv", "tp"),
            P("kv", "tp"),
            P("tp", "kv"),
        ),
        out_specs=P("grp", ("kv", "tp")),
        check_vma=False,
    )
```

```python
import jax
import jax.numpy as jnp
import numpy as np
from jax import lax
from jax.sharding import PartitionSpec as P

DK = 256
D = 4096
LANES = 128
NEAR = 4

RMS_EPS = 0.1
GN_EPS = 1.0
ROPE_BASE = 10000.0


def groups_near():
    n = lax.axis_size("kv")
    return [list(range(i, i + NEAR)) for i in range(0, n, NEAR)]


def groups_far():
    n = lax.axis_size("kv")
    return [list(range(i, n, NEAR)) for i in range(NEAR)]


def exchange(blocks, axis, groups=None):
    return lax.all_to_all(
        blocks, axis, split_axis=0, concat_axis=0, tiled=True, axis_index_groups=groups
    )


def spread(array, axis, peers, groups=None):
    return exchange(jnp.broadcast_to(array, (peers, *array.shape)), axis, groups)


def wide_sum(blocks):
    return jnp.sum(blocks.astype(jnp.float32), axis=0)


def hi_lo_rows(vector):
    high = lax.reduce_precision(vector, 8, 7)
    rows = jnp.stack([high, vector - high])
    return jnp.pad(rows, ((0, 6), (0, LANES - vector.shape[0])))


def near_blocks(array):
    return jnp.stack(
        [array[:, i * LANES : (i + 1) * LANES] for i in range(array.shape[1] // LANES)]
    )


def side(blocks):
    return jnp.concatenate([blocks[i] for i in range(blocks.shape[0])], axis=1)


def reduce_pair(first, second, extra=None, work=None, inputs=()):
    far = lax.axis_size("kv") // NEAR
    rows = first.shape[1]
    blocks = jnp.concatenate([first, second], axis=1)
    if extra is not None:
        tail = jnp.broadcast_to(hi_lo_rows(extra), (NEAR, 8, LANES))
        blocks = jnp.concatenate([blocks, tail], axis=1)
    blocks, inputs = lax.optimization_barrier((blocks.astype(jnp.bfloat16), inputs))
    got = wide_sum(exchange(blocks, "kv", groups_near()))
    if extra is not None:
        vector = got[2 * rows] + got[2 * rows + 1]
        got = jnp.concatenate([got[: 2 * rows], hi_lo_rows(vector[: extra.shape[0]])], axis=0)
    got = got.astype(jnp.bfloat16)
    if work is not None:
        got, inputs = lax.optimization_barrier((got, inputs))
        done = work(*inputs)
    got = spread(got, "kv", far, groups_far())
    if work is not None:
        got, done = lax.optimization_barrier((got, done))
    got = wide_sum(got)
    mine = got[: 2 * rows].astype(jnp.bfloat16)
    if extra is not None:
        vector = (got[2 * rows] + got[2 * rows + 1])[: extra.shape[0]]
        vector = lax.rsqrt(vector / D + RMS_EPS)
        mine, vector = lax.optimization_barrier((mine, vector))
    whole = spread(mine, "kv", NEAR, groups_near())
    if extra is not None:
        whole, vector = lax.optimization_barrier((whole, vector))
    outs = (whole[:, :rows].astype(jnp.float32), whole[:, rows:].astype(jnp.float32))
    if extra is None:
        return outs
    return (*outs, vector, done)


def near_columns(gate, up, stat, padded):
    quarter = gate.shape[1] // NEAR
    rest = padded - quarter
    zeros = jnp.zeros((gate.shape[0], rest), gate.dtype)
    fill = jnp.concatenate([stat[:, None].astype(gate.dtype), zeros[:, 1:]], axis=1)
    blocks = []
    for n in range(NEAR):
        own = slice(n * quarter, (n + 1) * quarter)
        blocks.append(jnp.concatenate([gate[:, own], fill, up[:, own], zeros], axis=1))
    return jnp.stack(blocks)


def with_gain(gain, w):
    return (gain[:, None] * w.astype(jnp.float32)).astype(jnp.bfloat16)


def rotate(halves, cosine, sine):
    outs = []
    for h in range(0, halves.shape[0], 2):
        a, b = halves[h], halves[h + 1]
        outs += [a * cosine - b * sine, a * sine + b * cosine]
    return outs


def gaps_to(lengths, span, at):
    slots = at * span + jnp.arange(span, dtype=jnp.int32)
    return (lengths[:, None] - slots[None, :]).astype(jnp.float32)


def decay_factors(gaps, log_decay):
    live = gaps > 0.0
    decays = jnp.exp(log_decay[None, :, None] * jnp.maximum(gaps, 0.0)[:, None, :])
    return jnp.where(live[:, None, :], decays, 0.0)


def cache_partial(query_low, decays, key_cache, value_cache, heads_here):
    batch_rows, _, span = decays.shape
    keys_here = key_cache.reshape(batch_rows, span, heads_here, DK)
    values_here = value_cache.reshape(batch_rows, span, heads_here, DK)
    scores = jnp.einsum("bphd,bhd->bhp", keys_here, query_low, preferred_element_type=jnp.float32)
    mixing = (scores * decays).astype(jnp.bfloat16)
    return jnp.einsum("bhp,bphd->bhd", mixing, values_here, preferred_element_type=jnp.float32)


def local(
    tokens,
    lengths,
    attn_gain,
    w_query,
    w_key,
    w_value,
    w_gate,
    log_decay,
    key_cache,
    value_cache,
    gn_gain,
    w_out,
    ffn_gain,
    w_ffn_gate,
    w_ffn_up,
    w_ffn_down,
):
    rows = tokens.shape[0]
    heads_here = log_decay.shape[0]
    tp = lax.axis_size("tp")
    own_width = tokens.shape[1]
    kv_at = lax.axis_index("kv")
    own_at = (lax.axis_index("tp") * own_width).astype(jnp.uint32)
    tokens, kv_at, own_at = lax.optimization_barrier((tokens, kv_at, own_at))
    gathered = spread(tokens, "tp", tp)
    w_joint = with_gain(attn_gain, jnp.concatenate([w_query, w_key], axis=1))
    gaps = gaps_to(lengths, key_cache.shape[1], kv_at)
    positions = lengths.astype(jnp.float32)
    gathered, w_joint, gaps, positions = lax.optimization_barrier(
        (gathered, w_joint, gaps, positions)
    )
    x = jnp.moveaxis(gathered, 0, 1).reshape(rows, tp * own_width)
    own_squares = jnp.sum(x.astype(jnp.float32) * x.astype(jnp.float32), axis=1)
    dot = lambda a, w: jnp.dot(a, w, preferred_element_type=jnp.float32)

    quarter = w_ffn_gate.shape[1] // NEAR
    padded = -(-(quarter + 1) // LANES) * LANES

    def ahead(
        x,
        positions,
        gaps,
        log_decay,
        attn_gain,
        w_value,
        w_gate,
        gn_gain,
        w_out,
        ffn_gain,
        w_fg,
        w_fu,
    ):
        half = DK // 2
        inverse = (ROPE_BASE ** (-np.arange(half) / half)).astype(np.float32)
        angles = positions[:, None] * inverse[None, :]
        return (
            jnp.cos(angles),
            jnp.sin(angles),
            decay_factors(gaps, log_decay),
            dot(x, with_gain(attn_gain, w_value)),
            dot(x, with_gain(attn_gain, w_gate)),
            x.astype(jnp.float32),
            with_gain(gn_gain, w_out),
            with_gain(ffn_gain, w_fg),
            with_gain(ffn_gain, w_fu),
        )

    joint = near_blocks(dot(x, w_joint))
    q_raw, k_raw, factor, made = reduce_pair(
        joint[:NEAR],
        joint[NEAR:],
        own_squares,
        ahead,
        (
            x,
            positions,
            gaps,
            log_decay,
            attn_gain,
            w_value,
            w_gate,
            gn_gain,
            w_out,
            ffn_gain,
            w_ffn_gate,
            w_ffn_up,
        ),
    )
    cosine, sine, decays, part_value, part_gate, x, out_gained, gate_gained, up_gained = made
    factor = factor[:, None]
    queries = [a * DK ** (-0.5) for a in rotate(q_raw * factor, cosine, sine)]
    keys = rotate(k_raw * factor, cosine, sine)
    cached = cache_partial(
        jnp.concatenate(queries, axis=1).astype(jnp.bfloat16).reshape(rows, heads_here, DK),
        decays,
        key_cache,
        value_cache,
        heads_here,
    )
    totals = []
    for h in range(heads_here):
        two = (2 * h, 2 * h + 1)
        own_dot = sum(jnp.sum(queries[n] * keys[n], axis=1, keepdims=True) for n in two)
        value = part_value[:, h * DK : (h + 1) * DK] * factor
        total = cached[:, h] + own_dot * value
        total = total - jnp.mean(total, axis=1, keepdims=True)
        totals += [total[:, :LANES], total[:, LANES:]]
    totals, gates = reduce_pair(jnp.stack(totals), near_blocks(part_gate * factor))
    gated = []
    for h in range(heads_here):
        a, b = totals[2 * h], totals[2 * h + 1]
        center = (jnp.sum(a, axis=1, keepdims=True) + jnp.sum(b, axis=1, keepdims=True)) / DK
        a, b = a - center, b - center
        spread_ = jnp.sum(a * a, axis=1, keepdims=True) + jnp.sum(b * b, axis=1, keepdims=True)
        scale = lax.rsqrt(spread_ / DK + GN_EPS)
        gated += [
            (jax.nn.silu(gates[2 * h]) * (a * scale)).astype(jnp.bfloat16),
            (jax.nn.silu(gates[2 * h + 1]) * (b * scale)).astype(jnp.bfloat16),
        ]
    gated = jnp.concatenate(gated, axis=1)
    mixed = dot(gated, out_gained).astype(jnp.bfloat16)
    mixed = wide_sum(spread(mixed, "tp", tp))
    resid = (x + mixed).astype(jnp.bfloat16)
    resid_wide = resid.astype(jnp.float32)
    mid_squares = jnp.sum(resid_wide * resid_wide, axis=1)
    blocks = near_columns(
        dot(resid, gate_gained).astype(jnp.bfloat16),
        dot(resid, up_gained).astype(jnp.bfloat16),
        mid_squares,
        padded,
    )
    got = wide_sum(exchange(blocks, "kv", groups_near()))
    got = wide_sum(
        lax.all_gather(got.astype(jnp.bfloat16), "kv", axis_index_groups=groups_far())
    )
    factor_mid = lax.rsqrt(got[:, quarter : quarter + 1] / D + RMS_EPS)
    hidden = jax.nn.silu(got[:, :padded] * factor_mid) * (got[:, padded:] * factor_mid)
    whole = spread(hidden.astype(jnp.bfloat16), "kv", NEAR, groups_near())
    hidden = side(whole[:, :, :quarter])
    down_part = dot(hidden, w_ffn_down).astype(jnp.bfloat16)
    down = wide_sum(spread(down_part, "tp", tp))
    return lax.dynamic_slice(
        (resid_wide + down).astype(jnp.bfloat16), (jnp.uint32(0), own_at), (rows, own_width)
    )


def solution(mesh):
    return jax.shard_map(
        local,
        mesh=mesh,
        in_specs=(
            P("grp", ("kv", "tp")),
            P("grp"),
            P("kv"),
            P("kv", "tp"),
            P("kv", "tp"),
            P("kv", "tp"),
            P("kv", "tp"),
            P("tp"),
            P("grp", "kv", "tp"),
            P("grp", "kv", "tp"),
            P("tp"),
            P("tp", "kv"),
            P("kv"),
            P("kv", "tp"),
            P("kv", "tp"),
            P("tp", "kv"),
        ),
        out_specs=P("grp", ("kv", "tp")),
        check_vma=False,
    )
```

```python
import jax
import jax.numpy as jnp
import numpy as np
from jax import lax
from jax.sharding import PartitionSpec as P

DK = 256
D = 4096
LANES = 128
NEAR = 4

RMS_EPS = 0.1
GN_EPS = 1.0
ROPE_BASE = 10000.0


def groups_near():
    n = lax.axis_size("kv")
    return [list(range(i, i + NEAR)) for i in range(0, n, NEAR)]


def groups_far():
    n = lax.axis_size("kv")
    return [list(range(i, n, NEAR)) for i in range(NEAR)]


def exchange(blocks, axis, groups=None):
    return lax.all_to_all(
        blocks, axis, split_axis=0, concat_axis=0, tiled=True, axis_index_groups=groups
    )


def spread(array, axis, peers, groups=None):
    return exchange(jnp.broadcast_to(array, (peers, *array.shape)), axis, groups)


def wide_sum(blocks):
    return jnp.sum(blocks.astype(jnp.float32), axis=0)


def hi_lo_rows(vector):
    high = lax.reduce_precision(vector, 8, 7)
    rows = jnp.stack([high, vector - high])
    return jnp.pad(rows, ((0, 6), (0, LANES - vector.shape[0])))


def near_blocks(array):
    return jnp.stack(
        [array[:, i * LANES : (i + 1) * LANES] for i in range(array.shape[1] // LANES)]
    )


def side(blocks):
    return jnp.concatenate([blocks[i] for i in range(blocks.shape[0])], axis=1)


def reduce_pair(first, second, extra=None, beside=()):
    far = lax.axis_size("kv") // NEAR
    rows = first.shape[1]
    blocks = jnp.concatenate([first, second], axis=1)
    if extra is not None:
        tail = jnp.broadcast_to(hi_lo_rows(extra), (NEAR, 8, LANES))
        blocks = jnp.concatenate([blocks, tail], axis=1)
    blocks, beside = lax.optimization_barrier((blocks.astype(jnp.bfloat16), beside))
    got = wide_sum(exchange(blocks, "kv", groups_near()))
    if extra is not None:
        vector = got[2 * rows] + got[2 * rows + 1]
        got = jnp.concatenate([got[: 2 * rows], hi_lo_rows(vector[: extra.shape[0]])], axis=0)
    got = wide_sum(spread(got.astype(jnp.bfloat16), "kv", far, groups_far()))
    mine = got[: 2 * rows].astype(jnp.bfloat16)
    if extra is not None:
        vector = (got[2 * rows] + got[2 * rows + 1])[: extra.shape[0]]
        vector = lax.rsqrt(vector / D + RMS_EPS)
        mine, vector = lax.optimization_barrier((mine, vector))
    whole = spread(mine, "kv", NEAR, groups_near())
    if extra is not None:
        whole, vector = lax.optimization_barrier((whole, vector))
    outs = (whole[:, :rows].astype(jnp.float32), whole[:, rows:].astype(jnp.float32))
    if extra is None:
        return outs
    return (*outs, vector, beside)


def near_columns(gate, up, stat, padded):
    quarter = gate.shape[1] // NEAR
    rest = padded - quarter
    zeros = jnp.zeros((gate.shape[0], rest), gate.dtype)
    fill = jnp.concatenate([stat[:, None].astype(gate.dtype), zeros[:, 1:]], axis=1)
    blocks = []
    for n in range(NEAR):
        own = slice(n * quarter, (n + 1) * quarter)
        blocks.append(jnp.concatenate([gate[:, own], fill, up[:, own], zeros], axis=1))
    return jnp.stack(blocks)


def with_gain(gain, w):
    return (gain[:, None] * w.astype(jnp.float32)).astype(jnp.bfloat16)


def rotate(halves, cosine, sine):
    outs = []
    for h in range(0, halves.shape[0], 2):
        a, b = halves[h], halves[h + 1]
        outs += [a * cosine - b * sine, a * sine + b * cosine]
    return outs


def gaps_to(lengths, span, at):
    slots = at * span + jnp.arange(span, dtype=jnp.int32)
    return lengths[:, None] - slots.astype(jnp.float32)[None, :]


def decay_factors(gaps, log_decay):
    live = gaps > 0.0
    decays = jnp.exp(log_decay[None, :, None] * jnp.maximum(gaps, 0.0)[:, None, :])
    return jnp.where(live[:, None, :], decays, 0.0)


def cache_partial(query_low, decays, key_cache, value_cache, heads_here):
    batch_rows, _, span = decays.shape
    keys_here = key_cache.reshape(batch_rows, span, heads_here, DK)
    values_here = value_cache.reshape(batch_rows, span, heads_here, DK)
    scores = jnp.einsum("bphd,bhd->bhp", keys_here, query_low, preferred_element_type=jnp.float32)
    mixing = (scores * decays).astype(jnp.bfloat16)
    return jnp.einsum("bhp,bphd->bhd", mixing, values_here, preferred_element_type=jnp.float32)


def local(
    tokens,
    lengths,
    attn_gain,
    w_query,
    w_key,
    w_value,
    w_gate,
    log_decay,
    key_cache,
    value_cache,
    gn_gain,
    w_out,
    ffn_gain,
    w_ffn_gate,
    w_ffn_up,
    w_ffn_down,
):
    rows = tokens.shape[0]
    heads_here = log_decay.shape[0]
    tp = lax.axis_size("tp")
    own_width = tokens.shape[1]
    kv_at = lax.axis_index("kv")
    own_at = (lax.axis_index("tp") * own_width).astype(jnp.uint32)
    tokens, kv_at, own_at = lax.optimization_barrier((tokens, kv_at, own_at))
    gathered = spread(tokens, "tp", tp)
    dot = lambda a, w: jnp.dot(a, w, preferred_element_type=jnp.float32)
    half = DK // 2
    inverse = (ROPE_BASE ** (-np.arange(half) / half)).astype(np.float32)
    positions = lax.optimization_barrier(lengths.astype(jnp.float32))
    angles = positions[:, None] * inverse[None, :]
    gaps = lax.optimization_barrier(gaps_to(positions, key_cache.shape[1], kv_at))
    made = (
        with_gain(attn_gain, jnp.concatenate([w_query, w_key, w_value, w_gate], axis=1)),
        with_gain(gn_gain, w_out),
        with_gain(ffn_gain, w_ffn_gate),
        with_gain(ffn_gain, w_ffn_up),
        jnp.cos(angles),
        jnp.sin(angles),
        decay_factors(gaps, log_decay),
    )
    gathered, made = lax.optimization_barrier((gathered, made))
    w_joint, out_gained, gate_gained, up_gained, cosine, sine, decays = made
    x = jnp.moveaxis(gathered, 0, 1).reshape(rows, tp * own_width)
    wide_x = x.astype(jnp.float32)
    own_squares = jnp.sum(wide_x * wide_x, axis=1)
    quarter = w_ffn_gate.shape[1] // NEAR
    padded = -(-(quarter + 1) // LANES) * LANES
    joint = dot(x, w_joint)
    width = heads_here * DK
    pairs = near_blocks(joint[:, : 2 * width])
    q_raw, k_raw, factor, (part_value, part_gate, x) = reduce_pair(
        pairs[:NEAR],
        pairs[NEAR:],
        own_squares,
        (joint[:, 2 * width : 3 * width], joint[:, 3 * width :], wide_x),
    )
    factor = factor[:, None]
    queries = [a * DK ** (-0.5) for a in rotate(q_raw * factor, cosine, sine)]
    keys = rotate(k_raw * factor, cosine, sine)
    cached = cache_partial(
        jnp.concatenate(queries, axis=1).astype(jnp.bfloat16).reshape(rows, heads_here, DK),
        decays,
        key_cache,
        value_cache,
        heads_here,
    )
    totals = []
    for h in range(heads_here):
        two = (2 * h, 2 * h + 1)
        own_dot = sum(jnp.sum(queries[n] * keys[n], axis=1, keepdims=True) for n in two)
        value = part_value[:, h * DK : (h + 1) * DK] * factor
        total = cached[:, h] + own_dot * value
        total = total - jnp.mean(total, axis=1, keepdims=True)
        totals += [total[:, :LANES], total[:, LANES:]]
    totals, gates = reduce_pair(jnp.stack(totals), near_blocks(part_gate * factor))
    gated = []
    for h in range(heads_here):
        a, b = totals[2 * h], totals[2 * h + 1]
        center = (jnp.sum(a, axis=1, keepdims=True) + jnp.sum(b, axis=1, keepdims=True)) / DK
        a, b = a - center, b - center
        spread_ = jnp.sum(a * a, axis=1, keepdims=True) + jnp.sum(b * b, axis=1, keepdims=True)
        scale = lax.rsqrt(spread_ / DK + GN_EPS)
        gated += [
            (jax.nn.silu(gates[2 * h]) * (a * scale)).astype(jnp.bfloat16),
            (jax.nn.silu(gates[2 * h + 1]) * (b * scale)).astype(jnp.bfloat16),
        ]
    gated = jnp.concatenate(gated, axis=1)
    mixed = dot(gated, out_gained).astype(jnp.bfloat16)
    mixed = wide_sum(spread(mixed, "tp", tp))
    resid = (x + mixed).astype(jnp.bfloat16)
    resid_wide = resid.astype(jnp.float32)
    mid_squares = jnp.sum(resid_wide * resid_wide, axis=1)
    blocks = near_columns(
        dot(resid, gate_gained).astype(jnp.bfloat16),
        dot(resid, up_gained).astype(jnp.bfloat16),
        mid_squares,
        padded,
    )
    got = wide_sum(exchange(blocks, "kv", groups_near()))
    got = wide_sum(
        lax.all_gather(got.astype(jnp.bfloat16), "kv", axis_index_groups=groups_far())
    )
    factor_mid = lax.rsqrt(got[:, quarter : quarter + 1] / D + RMS_EPS)
    hidden = jax.nn.silu(got[:, :padded] * factor_mid) * (got[:, padded:] * factor_mid)
    whole = spread(hidden.astype(jnp.bfloat16), "kv", NEAR, groups_near())
    hidden = side(whole[:, :, :quarter])
    down_part = dot(hidden, w_ffn_down).astype(jnp.bfloat16)
    down = wide_sum(spread(down_part, "tp", tp))
    return lax.dynamic_slice(
        (resid_wide + down).astype(jnp.bfloat16), (jnp.uint32(0), own_at), (rows, own_width)
    )


def solution(mesh):
    return jax.shard_map(
        local,
        mesh=mesh,
        in_specs=(
            P("grp", ("kv", "tp")),
            P("grp"),
            P("kv"),
            P("kv", "tp"),
            P("kv", "tp"),
            P("kv", "tp"),
            P("kv", "tp"),
            P("tp"),
            P("grp", "kv", "tp"),
            P("grp", "kv", "tp"),
            P("tp"),
            P("tp", "kv"),
            P("kv"),
            P("kv", "tp"),
            P("kv", "tp"),
            P("tp", "kv"),
        ),
        out_specs=P("grp", ("kv", "tp")),
        check_vma=False,
    )
```

```python
import jax
import jax.numpy as jnp
from jax import lax
from jax.sharding import PartitionSpec as P

DK = 256
D = 4096
LANES = 128
NEAR = 4

RMS_EPS = 0.1
GN_EPS = 1.0
ROPE_BASE = 10000.0


def groups_near():
    n = lax.axis_size("kv")
    return [list(range(i, i + NEAR)) for i in range(0, n, NEAR)]


def groups_far():
    n = lax.axis_size("kv")
    return [list(range(i, n, NEAR)) for i in range(NEAR)]


def exchange(blocks, axis, groups=None):
    return lax.all_to_all(
        blocks, axis, split_axis=0, concat_axis=0, tiled=True, axis_index_groups=groups
    )


def spread(array, axis, peers, groups=None):
    return exchange(jnp.broadcast_to(array, (peers, *array.shape)), axis, groups)


def wide_sum(blocks):
    return jnp.sum(blocks.astype(jnp.float32), axis=0)


def hi_lo_rows(vector):
    high = lax.reduce_precision(vector, 8, 7)
    rows = jnp.stack([high, vector - high])
    return jnp.pad(rows, ((0, 6), (0, LANES - vector.shape[0])))


def near_blocks(array):
    return jnp.stack(
        [array[:, i * LANES : (i + 1) * LANES] for i in range(array.shape[1] // LANES)]
    )


def side(blocks):
    return jnp.concatenate([blocks[i] for i in range(blocks.shape[0])], axis=1)


def reduce_pair(first, second, extra=None, beside=()):
    far = lax.axis_size("kv") // NEAR
    rows = first.shape[1]
    blocks = jnp.concatenate([first, second], axis=1)
    if extra is not None:
        tail = jnp.broadcast_to(hi_lo_rows(extra), (NEAR, 8, LANES))
        blocks = jnp.concatenate([blocks, tail], axis=1)
    blocks, beside = lax.optimization_barrier((blocks.astype(jnp.bfloat16), beside))
    got = wide_sum(exchange(blocks, "kv", groups_near()))
    if extra is not None:
        vector = got[2 * rows] + got[2 * rows + 1]
        got = jnp.concatenate([got[: 2 * rows], hi_lo_rows(vector[: extra.shape[0]])], axis=0)
    got = wide_sum(spread(got.astype(jnp.bfloat16), "kv", far, groups_far()))
    mine = got[: 2 * rows].astype(jnp.bfloat16)
    if extra is not None:
        vector = (got[2 * rows] + got[2 * rows + 1])[: extra.shape[0]]
        vector = lax.rsqrt(vector / D + RMS_EPS)
        mine, vector = lax.optimization_barrier((mine, vector))
    whole = spread(mine, "kv", NEAR, groups_near())
    if extra is not None:
        whole, vector = lax.optimization_barrier((whole, vector))
    outs = (whole[:, :rows].astype(jnp.float32), whole[:, rows:].astype(jnp.float32))
    if extra is None:
        return outs
    return (*outs, vector, beside)


def near_columns(gate, up, stat, padded):
    quarter = gate.shape[1] // NEAR
    rest = padded - quarter
    zeros = jnp.zeros((gate.shape[0], rest), gate.dtype)
    fill = jnp.concatenate([stat[:, None].astype(gate.dtype), zeros[:, 1:]], axis=1)
    blocks = []
    for n in range(NEAR):
        own = slice(n * quarter, (n + 1) * quarter)
        blocks.append(jnp.concatenate([gate[:, own], fill, up[:, own], zeros], axis=1))
    return jnp.stack(blocks)


def with_gain(gain, w):
    return (gain[:, None] * w.astype(jnp.float32)).astype(jnp.bfloat16)


def rotate(halves, cosine, sine):
    outs = []
    for h in range(0, halves.shape[0], 2):
        a, b = halves[h], halves[h + 1]
        outs += [a * cosine - b * sine, a * sine + b * cosine]
    return outs


def gaps_to(lengths, span, at):
    slots = at * span + jnp.arange(span, dtype=jnp.int32)
    return lengths[:, None] - slots.astype(jnp.float32)[None, :]


def decay_factors(gaps, log_decay):
    live = gaps > 0.0
    decays = jnp.exp(log_decay[None, :, None] * jnp.maximum(gaps, 0.0)[:, None, :])
    return jnp.where(live[:, None, :], decays, 0.0)


def cache_partial(query_low, decays, key_cache, value_cache, heads_here):
    batch_rows, _, span = decays.shape
    keys_here = key_cache.reshape(batch_rows, span, heads_here, DK)
    values_here = value_cache.reshape(batch_rows, span, heads_here, DK)
    scores = jnp.einsum("bphd,bhd->bhp", keys_here, query_low, preferred_element_type=jnp.float32)
    mixing = (scores * decays).astype(jnp.bfloat16)
    return jnp.einsum("bhp,bphd->bhd", mixing, values_here, preferred_element_type=jnp.float32)


def local(
    tokens,
    lengths,
    attn_gain,
    w_query,
    w_key,
    w_value,
    w_gate,
    log_decay,
    key_cache,
    value_cache,
    gn_gain,
    w_out,
    ffn_gain,
    w_ffn_gate,
    w_ffn_up,
    w_ffn_down,
):
    rows = tokens.shape[0]
    heads_here = log_decay.shape[0]
    tp = lax.axis_size("tp")
    own_width = tokens.shape[1]
    kv_at = lax.axis_index("kv")
    own_at = (lax.axis_index("tp") * own_width).astype(jnp.uint32)
    tokens, kv_at, own_at = lax.optimization_barrier((tokens, kv_at, own_at))
    gathered = spread(tokens, "tp", tp)
    dot = lambda a, w: jnp.dot(a, w, preferred_element_type=jnp.float32)
    half = DK // 2
    inverse = ROPE_BASE ** (-jnp.arange(half, dtype=jnp.float32) / half)
    positions = lax.optimization_barrier(lengths.astype(jnp.float32))
    angles = positions[:, None] * inverse[None, :]
    gaps = lax.optimization_barrier(gaps_to(positions, key_cache.shape[1], kv_at))
    made = (
        with_gain(attn_gain, jnp.concatenate([w_query, w_key, w_value, w_gate], axis=1)),
        with_gain(gn_gain, w_out),
        with_gain(ffn_gain, w_ffn_gate),
        with_gain(ffn_gain, w_ffn_up),
        jnp.cos(angles),
        jnp.sin(angles),
        decay_factors(gaps, log_decay),
    )
    gathered, made = lax.optimization_barrier((gathered, made))
    w_joint, out_gained, gate_gained, up_gained, cosine, sine, decays = made
    x = jnp.moveaxis(gathered, 0, 1).reshape(rows, tp * own_width)
    wide_x = x.astype(jnp.float32)
    own_squares = jnp.sum(wide_x * wide_x, axis=1)
    quarter = w_ffn_gate.shape[1] // NEAR
    padded = -(-(quarter + 1) // LANES) * LANES
    joint = dot(x, w_joint)
    width = heads_here * DK
    pairs = near_blocks(joint[:, : 2 * width])
    q_raw, k_raw, factor, (part_value, part_gate, x) = reduce_pair(
        pairs[:NEAR],
        pairs[NEAR:],
        own_squares,
        (joint[:, 2 * width : 3 * width], joint[:, 3 * width :], wide_x),
    )
    factor = factor[:, None]
    queries = [a * DK ** (-0.5) for a in rotate(q_raw * factor, cosine, sine)]
    keys = rotate(k_raw * factor, cosine, sine)
    cached = cache_partial(
        jnp.concatenate(queries, axis=1).astype(jnp.bfloat16).reshape(rows, heads_here, DK),
        decays,
        key_cache,
        value_cache,
        heads_here,
    )
    totals = []
    for h in range(heads_here):
        two = (2 * h, 2 * h + 1)
        own_dot = sum(jnp.sum(queries[n] * keys[n], axis=1, keepdims=True) for n in two)
        value = part_value[:, h * DK : (h + 1) * DK] * factor
        total = cached[:, h] + own_dot * value
        total = total - jnp.mean(total, axis=1, keepdims=True)
        totals += [total[:, :LANES], total[:, LANES:]]
    totals, gates = reduce_pair(jnp.stack(totals), near_blocks(part_gate * factor))
    gated = []
    for h in range(heads_here):
        a, b = totals[2 * h], totals[2 * h + 1]
        center = (jnp.sum(a, axis=1, keepdims=True) + jnp.sum(b, axis=1, keepdims=True)) / DK
        a, b = a - center, b - center
        spread_ = jnp.sum(a * a, axis=1, keepdims=True) + jnp.sum(b * b, axis=1, keepdims=True)
        scale = lax.rsqrt(spread_ / DK + GN_EPS)
        gated += [
            (jax.nn.silu(gates[2 * h]) * (a * scale)).astype(jnp.bfloat16),
            (jax.nn.silu(gates[2 * h + 1]) * (b * scale)).astype(jnp.bfloat16),
        ]
    gated = jnp.concatenate(gated, axis=1)
    mixed = dot(gated, out_gained).astype(jnp.bfloat16)
    mixed = wide_sum(spread(mixed, "tp", tp))
    resid = (x + mixed).astype(jnp.bfloat16)
    resid_wide = resid.astype(jnp.float32)
    mid_squares = jnp.sum(resid_wide * resid_wide, axis=1)
    blocks = near_columns(
        dot(resid, gate_gained).astype(jnp.bfloat16),
        dot(resid, up_gained).astype(jnp.bfloat16),
        mid_squares,
        padded,
    )
    got = wide_sum(exchange(blocks, "kv", groups_near()))
    got = wide_sum(
        lax.all_gather(got.astype(jnp.bfloat16), "kv", axis_index_groups=groups_far())
    )
    factor_mid = lax.rsqrt(got[:, quarter : quarter + 1] / D + RMS_EPS)
    hidden = jax.nn.silu(got[:, :padded] * factor_mid) * (got[:, padded:] * factor_mid)
    whole = spread(hidden.astype(jnp.bfloat16), "kv", NEAR, groups_near())
    hidden = side(whole[:, :, :quarter])
    down_part = dot(hidden, w_ffn_down).astype(jnp.bfloat16)
    down = wide_sum(spread(down_part, "tp", tp))
    return lax.dynamic_slice(
        (resid_wide + down).astype(jnp.bfloat16), (jnp.uint32(0), own_at), (rows, own_width)
    )


def solution(mesh):
    return jax.shard_map(
        local,
        mesh=mesh,
        in_specs=(
            P("grp", ("kv", "tp")),
            P("grp"),
            P("kv"),
            P("kv", "tp"),
            P("kv", "tp"),
            P("kv", "tp"),
            P("kv", "tp"),
            P("tp"),
            P("grp", "kv", "tp"),
            P("grp", "kv", "tp"),
            P("tp"),
            P("tp", "kv"),
            P("kv"),
            P("kv", "tp"),
            P("kv", "tp"),
            P("tp", "kv"),
        ),
        out_specs=P("grp", ("kv", "tp")),
        check_vma=False,
    )
```

```python
import jax
import jax.numpy as jnp
from jax import lax
from jax.sharding import PartitionSpec as P

DK = 256
D = 4096
LANES = 128
NEAR = 4

RMS_EPS = 0.1
GN_EPS = 1.0
ROPE_BASE = 10000.0


def groups_near():
    n = lax.axis_size("kv")
    return [list(range(i, i + NEAR)) for i in range(0, n, NEAR)]


def groups_far():
    n = lax.axis_size("kv")
    return [list(range(i, n, NEAR)) for i in range(NEAR)]


def exchange(blocks, axis, groups=None):
    return lax.all_to_all(
        blocks, axis, split_axis=0, concat_axis=0, tiled=True, axis_index_groups=groups
    )


def spread(array, axis, peers, groups=None):
    return exchange(jnp.broadcast_to(array, (peers, *array.shape)), axis, groups)


def wide_sum(blocks):
    return jnp.sum(blocks.astype(jnp.float32), axis=0)


def hi_lo_rows(vector):
    high = lax.reduce_precision(vector, 8, 7)
    rows = jnp.stack([high, vector - high])
    return jnp.pad(rows, ((0, 6), (0, LANES - vector.shape[0])))


def near_blocks(array):
    return jnp.stack(
        [array[:, i * LANES : (i + 1) * LANES] for i in range(array.shape[1] // LANES)]
    )


def side(blocks):
    return jnp.concatenate([blocks[i] for i in range(blocks.shape[0])], axis=1)


def reduce_pair(first, second, extra=None, beside=()):
    far = lax.axis_size("kv") // NEAR
    rows = first.shape[1]
    blocks = jnp.concatenate([first, second], axis=1)
    if extra is not None:
        tail = jnp.broadcast_to(hi_lo_rows(extra), (NEAR, 8, LANES))
        blocks = jnp.concatenate([blocks, tail], axis=1)
    blocks, beside = lax.optimization_barrier((blocks.astype(jnp.bfloat16), beside))
    got = wide_sum(exchange(blocks, "kv", groups_near()))
    if extra is not None:
        vector = got[2 * rows] + got[2 * rows + 1]
        got = jnp.concatenate([got[: 2 * rows], hi_lo_rows(vector[: extra.shape[0]])], axis=0)
    got = wide_sum(spread(got.astype(jnp.bfloat16), "kv", far, groups_far()))
    mine = got[: 2 * rows].astype(jnp.bfloat16)
    if extra is not None:
        vector = (got[2 * rows] + got[2 * rows + 1])[: extra.shape[0]]
        vector = lax.rsqrt(vector / D + RMS_EPS)
        mine, vector = lax.optimization_barrier((mine, vector))
    whole = spread(mine, "kv", NEAR, groups_near())
    if extra is not None:
        whole, vector = lax.optimization_barrier((whole, vector))
    outs = (whole[:, :rows].astype(jnp.float32), whole[:, rows:].astype(jnp.float32))
    if extra is None:
        return outs
    return (*outs, vector, beside)


def near_columns(gate, up, stat, padded):
    quarter = gate.shape[1] // NEAR
    rest = padded - quarter
    zeros = jnp.zeros((gate.shape[0], rest), gate.dtype)
    fill = jnp.concatenate([stat[:, None].astype(gate.dtype), zeros[:, 1:]], axis=1)
    blocks = []
    for n in range(NEAR):
        own = slice(n * quarter, (n + 1) * quarter)
        blocks.append(jnp.concatenate([gate[:, own], fill, up[:, own], zeros], axis=1))
    return jnp.stack(blocks)


def with_gain(gain, w):
    return (gain[:, None] * w.astype(jnp.float32)).astype(jnp.bfloat16)


def rotate(halves, cosine, sine):
    outs = []
    for h in range(0, halves.shape[0], 2):
        a, b = halves[h], halves[h + 1]
        outs += [a * cosine - b * sine, a * sine + b * cosine]
    return outs


def gaps_to(lengths, span, at):
    slots = at * span + jnp.arange(span, dtype=jnp.int32)
    return lengths[:, None] - slots.astype(jnp.float32)[None, :]


def decay_factors(gaps, log_decay):
    live = gaps > 0.0
    decays = jnp.exp(log_decay[None, :, None] * jnp.maximum(gaps, 0.0)[:, None, :])
    return jnp.where(live[:, None, :], decays, 0.0)


def cache_partial(query_low, decays, key_cache, value_cache, heads_here):
    batch_rows, _, span = decays.shape
    keys_here = key_cache.reshape(batch_rows, span, heads_here, DK)
    values_here = value_cache.reshape(batch_rows, span, heads_here, DK)
    scores = jnp.einsum("bphd,bhd->bhp", keys_here, query_low, preferred_element_type=jnp.float32)
    mixing = (scores * decays).astype(jnp.bfloat16)
    return jnp.einsum("bhp,bphd->bhd", mixing, values_here, preferred_element_type=jnp.float32)


def local(
    tokens,
    lengths,
    attn_gain,
    w_query,
    w_key,
    w_value,
    w_gate,
    log_decay,
    key_cache,
    value_cache,
    gn_gain,
    w_out,
    ffn_gain,
    w_ffn_gate,
    w_ffn_up,
    w_ffn_down,
):
    rows = tokens.shape[0]
    heads_here = log_decay.shape[0]
    tp = lax.axis_size("tp")
    own_width = tokens.shape[1]
    kv_at = lax.axis_index("kv")
    own_at = (lax.axis_index("tp") * own_width).astype(jnp.uint32)
    tokens, kv_at, own_at = lax.optimization_barrier((tokens, kv_at, own_at))
    gathered = spread(tokens, "tp", tp)
    dot = lambda a, w: jnp.dot(a, w, preferred_element_type=jnp.float32)
    half = DK // 2
    inverse = ROPE_BASE ** (-jnp.arange(half, dtype=jnp.float32) / half)
    w_joint = with_gain(attn_gain, jnp.concatenate([w_query, w_key, w_value, w_gate], axis=1))
    w_joint, ffn_gain, w_ffn_gate, w_ffn_up = lax.optimization_barrier(
        (w_joint, ffn_gain, w_ffn_gate, w_ffn_up)
    )
    ffn_gained = (with_gain(ffn_gain, w_ffn_gate), with_gain(ffn_gain, w_ffn_up))
    ffn_gained, lengths = lax.optimization_barrier((ffn_gained, lengths))
    positions = lax.optimization_barrier(lengths.astype(jnp.float32))
    angles = positions[:, None] * inverse[None, :]
    gaps = lax.optimization_barrier(gaps_to(positions, key_cache.shape[1], kv_at))
    decays = decay_factors(gaps, log_decay)
    decays, gn_gain, w_out = lax.optimization_barrier((decays, gn_gain, w_out))
    made = (
        w_joint,
        with_gain(gn_gain, w_out),
        *ffn_gained,
        jnp.cos(angles),
        jnp.sin(angles),
        decays,
    )
    gathered, made = lax.optimization_barrier((gathered, made))
    w_joint, out_gained, gate_gained, up_gained, cosine, sine, decays = made
    x = jnp.moveaxis(gathered, 0, 1).reshape(rows, tp * own_width)
    wide_x = x.astype(jnp.float32)
    own_squares = jnp.sum(wide_x * wide_x, axis=1)
    quarter = w_ffn_gate.shape[1] // NEAR
    padded = -(-(quarter + 1) // LANES) * LANES
    joint = dot(x, w_joint)
    width = heads_here * DK
    pairs = near_blocks(joint[:, : 2 * width])
    q_raw, k_raw, factor, (part_value, part_gate, x) = reduce_pair(
        pairs[:NEAR],
        pairs[NEAR:],
        own_squares,
        (joint[:, 2 * width : 3 * width], joint[:, 3 * width :], wide_x),
    )
    factor = factor[:, None]
    queries = [a * DK ** (-0.5) for a in rotate(q_raw * factor, cosine, sine)]
    keys = rotate(k_raw * factor, cosine, sine)
    cached = cache_partial(
        jnp.concatenate(queries, axis=1).astype(jnp.bfloat16).reshape(rows, heads_here, DK),
        decays,
        key_cache,
        value_cache,
        heads_here,
    )
    totals = []
    for h in range(heads_here):
        two = (2 * h, 2 * h + 1)
        own_dot = sum(jnp.sum(queries[n] * keys[n], axis=1, keepdims=True) for n in two)
        value = part_value[:, h * DK : (h + 1) * DK] * factor
        total = cached[:, h] + own_dot * value
        total = total - jnp.mean(total, axis=1, keepdims=True)
        totals += [total[:, :LANES], total[:, LANES:]]
    totals, gates = reduce_pair(jnp.stack(totals), near_blocks(part_gate * factor))
    gated = []
    for h in range(heads_here):
        a, b = totals[2 * h], totals[2 * h + 1]
        center = (jnp.sum(a, axis=1, keepdims=True) + jnp.sum(b, axis=1, keepdims=True)) / DK
        a, b = a - center, b - center
        spread_ = jnp.sum(a * a, axis=1, keepdims=True) + jnp.sum(b * b, axis=1, keepdims=True)
        scale = lax.rsqrt(spread_ / DK + GN_EPS)
        gated += [
            (jax.nn.silu(gates[2 * h]) * (a * scale)).astype(jnp.bfloat16),
            (jax.nn.silu(gates[2 * h + 1]) * (b * scale)).astype(jnp.bfloat16),
        ]
    gated = jnp.concatenate(gated, axis=1)
    mixed = dot(gated, out_gained).astype(jnp.bfloat16)
    mixed = wide_sum(spread(mixed, "tp", tp))
    resid = (x + mixed).astype(jnp.bfloat16)
    resid_wide = resid.astype(jnp.float32)
    mid_squares = jnp.sum(resid_wide * resid_wide, axis=1)
    blocks = near_columns(
        dot(resid, gate_gained).astype(jnp.bfloat16),
        dot(resid, up_gained).astype(jnp.bfloat16),
        mid_squares,
        padded,
    )
    got = wide_sum(exchange(blocks, "kv", groups_near()))
    got = wide_sum(
        lax.all_gather(got.astype(jnp.bfloat16), "kv", axis_index_groups=groups_far())
    )
    factor_mid = lax.rsqrt(got[:, quarter : quarter + 1] / D + RMS_EPS)
    hidden = jax.nn.silu(got[:, :padded] * factor_mid) * (got[:, padded:] * factor_mid)
    whole = spread(hidden.astype(jnp.bfloat16), "kv", NEAR, groups_near())
    hidden = side(whole[:, :, :quarter])
    down_part = dot(hidden, w_ffn_down).astype(jnp.bfloat16)
    down = wide_sum(spread(down_part, "tp", tp))
    return lax.dynamic_slice(
        (resid_wide + down).astype(jnp.bfloat16), (jnp.uint32(0), own_at), (rows, own_width)
    )


def solution(mesh):
    return jax.shard_map(
        local,
        mesh=mesh,
        in_specs=(
            P("grp", ("kv", "tp")),
            P("grp"),
            P("kv"),
            P("kv", "tp"),
            P("kv", "tp"),
            P("kv", "tp"),
            P("kv", "tp"),
            P("tp"),
            P("grp", "kv", "tp"),
            P("grp", "kv", "tp"),
            P("tp"),
            P("tp", "kv"),
            P("kv"),
            P("kv", "tp"),
            P("kv", "tp"),
            P("tp", "kv"),
        ),
        out_specs=P("grp", ("kv", "tp")),
        check_vma=False,
    )
```

```python
import jax
import jax.numpy as jnp
from jax import lax
from jax.sharding import PartitionSpec as P

DK = 256
D = 4096
LANES = 128
NEAR = 4

RMS_EPS = 0.1
GN_EPS = 1.0
ROPE_BASE = 10000.0


def groups_near():
    n = lax.axis_size("kv")
    return [list(range(i, i + NEAR)) for i in range(0, n, NEAR)]


def groups_far():
    n = lax.axis_size("kv")
    return [list(range(i, n, NEAR)) for i in range(NEAR)]


def exchange(blocks, axis, groups=None):
    return lax.all_to_all(
        blocks, axis, split_axis=0, concat_axis=0, tiled=True, axis_index_groups=groups
    )


def spread(array, axis, peers, groups=None):
    return exchange(jnp.broadcast_to(array, (peers, *array.shape)), axis, groups)


def wide_sum(blocks):
    return jnp.sum(blocks.astype(jnp.float32), axis=0)


def hi_lo_rows(vector):
    high = lax.reduce_precision(vector, 8, 7)
    rows = jnp.stack([high, vector - high])
    return jnp.pad(rows, ((0, 6), (0, LANES - vector.shape[0])))


def near_blocks(array):
    return jnp.stack(
        [array[:, i * LANES : (i + 1) * LANES] for i in range(array.shape[1] // LANES)]
    )


def side(blocks):
    return jnp.concatenate([blocks[i] for i in range(blocks.shape[0])], axis=1)


def reduce_pair(first, second, extra=None, beside=()):
    far = lax.axis_size("kv") // NEAR
    rows = first.shape[1]
    blocks = jnp.concatenate([first, second], axis=1)
    if extra is not None:
        tail = jnp.broadcast_to(hi_lo_rows(extra), (NEAR, 8, LANES))
        blocks = jnp.concatenate([blocks, tail], axis=1)
    blocks, beside = lax.optimization_barrier((blocks.astype(jnp.bfloat16), beside))
    got = wide_sum(exchange(blocks, "kv", groups_near()))
    if extra is not None:
        vector = got[2 * rows] + got[2 * rows + 1]
        got = jnp.concatenate([got[: 2 * rows], hi_lo_rows(vector[: extra.shape[0]])], axis=0)
    got = wide_sum(spread(got.astype(jnp.bfloat16), "kv", far, groups_far()))
    mine = got[: 2 * rows].astype(jnp.bfloat16)
    if extra is not None:
        vector = (got[2 * rows] + got[2 * rows + 1])[: extra.shape[0]]
        vector = lax.rsqrt(vector / D + RMS_EPS)
        mine, vector = lax.optimization_barrier((mine, vector))
    whole = spread(mine, "kv", NEAR, groups_near())
    if extra is not None:
        whole, vector = lax.optimization_barrier((whole, vector))
    outs = (whole[:, :rows].astype(jnp.float32), whole[:, rows:].astype(jnp.float32))
    if extra is None:
        return outs
    return (*outs, vector, beside)


def near_columns(gate, up, stat, padded):
    quarter = gate.shape[1] // NEAR
    rest = padded - quarter
    zeros = jnp.zeros((gate.shape[0], rest), gate.dtype)
    fill = jnp.concatenate([stat[:, None].astype(gate.dtype), zeros[:, 1:]], axis=1)
    blocks = []
    for n in range(NEAR):
        own = slice(n * quarter, (n + 1) * quarter)
        blocks.append(jnp.concatenate([gate[:, own], fill, up[:, own], zeros], axis=1))
    return jnp.stack(blocks)


def with_gain(gain, w):
    return (gain[:, None] * w.astype(jnp.float32)).astype(jnp.bfloat16)


def rotate(halves, cosine, sine):
    outs = []
    for h in range(0, halves.shape[0], 2):
        a, b = halves[h], halves[h + 1]
        outs += [a * cosine - b * sine, a * sine + b * cosine]
    return outs


def gaps_to(lengths, span, at):
    slots = at * span + jnp.arange(span, dtype=jnp.int32)
    return lengths[:, None] - slots.astype(jnp.float32)[None, :]


def decay_factors(gaps, log_decay):
    live = gaps > 0.0
    decays = jnp.exp(log_decay[None, :, None] * jnp.maximum(gaps, 0.0)[:, None, :])
    return jnp.where(live[:, None, :], decays, 0.0)


def cache_partial(query_low, decays, key_cache, value_cache, heads_here):
    batch_rows, _, span = decays.shape
    keys_here = key_cache.reshape(batch_rows, span, heads_here, DK)
    values_here = value_cache.reshape(batch_rows, span, heads_here, DK)
    scores = jnp.einsum("bphd,bhd->bhp", keys_here, query_low, preferred_element_type=jnp.float32)
    mixing = (scores * decays).astype(jnp.bfloat16)
    return jnp.einsum("bhp,bphd->bhd", mixing, values_here, preferred_element_type=jnp.float32)


def local(
    tokens,
    lengths,
    attn_gain,
    w_query,
    w_key,
    w_value,
    w_gate,
    log_decay,
    key_cache,
    value_cache,
    gn_gain,
    w_out,
    ffn_gain,
    w_ffn_gate,
    w_ffn_up,
    w_ffn_down,
):
    rows = tokens.shape[0]
    heads_here = log_decay.shape[0]
    tp = lax.axis_size("tp")
    own_width = tokens.shape[1]
    kv_at = lax.axis_index("kv")
    own_at = (lax.axis_index("tp") * own_width).astype(jnp.uint32)
    tokens, kv_at, own_at = lax.optimization_barrier((tokens, kv_at, own_at))
    gathered = spread(tokens, "tp", tp)
    dot = lambda a, w: jnp.dot(a, w, preferred_element_type=jnp.float32)
    half = DK // 2
    inverse = ROPE_BASE ** (-jnp.arange(half, dtype=jnp.float32) / half)
    w_joint = with_gain(attn_gain, jnp.concatenate([w_query, w_key, w_value, w_gate], axis=1))
    w_joint, ffn_gain, w_ffn_gate, w_ffn_up, lengths, log_decay, gn_gain, w_out = (
        lax.optimization_barrier(
            (w_joint, ffn_gain, w_ffn_gate, w_ffn_up, lengths, log_decay, gn_gain, w_out)
        )
    )
    ffn_gained = (with_gain(ffn_gain, w_ffn_gate), with_gain(ffn_gain, w_ffn_up))
    positions = lax.optimization_barrier(lengths.astype(jnp.float32))
    angles = positions[:, None] * inverse[None, :]
    gaps = lax.optimization_barrier(gaps_to(positions, key_cache.shape[1], kv_at))
    decays = decay_factors(gaps, log_decay)
    made = (
        w_joint,
        with_gain(gn_gain, w_out),
        *ffn_gained,
        jnp.cos(angles),
        jnp.sin(angles),
        decays,
    )
    gathered, made = lax.optimization_barrier((gathered, made))
    w_joint, out_gained, gate_gained, up_gained, cosine, sine, decays = made
    x = jnp.moveaxis(gathered, 0, 1).reshape(rows, tp * own_width)
    wide_x = x.astype(jnp.float32)
    own_squares = jnp.sum(wide_x * wide_x, axis=1)
    quarter = w_ffn_gate.shape[1] // NEAR
    padded = -(-(quarter + 1) // LANES) * LANES
    joint = dot(x, w_joint)
    width = heads_here * DK
    pairs = near_blocks(joint[:, : 2 * width])
    q_raw, k_raw, factor, (part_value, part_gate, x) = reduce_pair(
        pairs[:NEAR],
        pairs[NEAR:],
        own_squares,
        (joint[:, 2 * width : 3 * width], joint[:, 3 * width :], wide_x),
    )
    factor = factor[:, None]
    queries = [a * DK ** (-0.5) for a in rotate(q_raw * factor, cosine, sine)]
    keys = rotate(k_raw * factor, cosine, sine)
    cached = cache_partial(
        jnp.concatenate(queries, axis=1).astype(jnp.bfloat16).reshape(rows, heads_here, DK),
        decays,
        key_cache,
        value_cache,
        heads_here,
    )
    totals = []
    for h in range(heads_here):
        two = (2 * h, 2 * h + 1)
        own_dot = sum(jnp.sum(queries[n] * keys[n], axis=1, keepdims=True) for n in two)
        value = part_value[:, h * DK : (h + 1) * DK] * factor
        total = cached[:, h] + own_dot * value
        total = total - jnp.mean(total, axis=1, keepdims=True)
        totals += [total[:, :LANES], total[:, LANES:]]
    totals, gates = reduce_pair(jnp.stack(totals), near_blocks(part_gate * factor))
    gated = []
    for h in range(heads_here):
        a, b = totals[2 * h], totals[2 * h + 1]
        center = (jnp.sum(a, axis=1, keepdims=True) + jnp.sum(b, axis=1, keepdims=True)) / DK
        a, b = a - center, b - center
        spread_ = jnp.sum(a * a, axis=1, keepdims=True) + jnp.sum(b * b, axis=1, keepdims=True)
        scale = lax.rsqrt(spread_ / DK + GN_EPS)
        gated += [
            (jax.nn.silu(gates[2 * h]) * (a * scale)).astype(jnp.bfloat16),
            (jax.nn.silu(gates[2 * h + 1]) * (b * scale)).astype(jnp.bfloat16),
        ]
    gated = jnp.concatenate(gated, axis=1)
    mixed = dot(gated, out_gained).astype(jnp.bfloat16)
    mixed = wide_sum(spread(mixed, "tp", tp))
    resid = (x + mixed).astype(jnp.bfloat16)
    resid_wide = resid.astype(jnp.float32)
    mid_squares = jnp.sum(resid_wide * resid_wide, axis=1)
    blocks = near_columns(
        dot(resid, gate_gained).astype(jnp.bfloat16),
        dot(resid, up_gained).astype(jnp.bfloat16),
        mid_squares,
        padded,
    )
    got = wide_sum(exchange(blocks, "kv", groups_near()))
    got = wide_sum(
        lax.all_gather(got.astype(jnp.bfloat16), "kv", axis_index_groups=groups_far())
    )
    factor_mid = lax.rsqrt(got[:, quarter : quarter + 1] / D + RMS_EPS)
    hidden = jax.nn.silu(got[:, :padded] * factor_mid) * (got[:, padded:] * factor_mid)
    whole = spread(hidden.astype(jnp.bfloat16), "kv", NEAR, groups_near())
    hidden = side(whole[:, :, :quarter])
    down_part = dot(hidden, w_ffn_down).astype(jnp.bfloat16)
    down = wide_sum(spread(down_part, "tp", tp))
    return lax.dynamic_slice(
        (resid_wide + down).astype(jnp.bfloat16), (jnp.uint32(0), own_at), (rows, own_width)
    )


def solution(mesh):
    return jax.shard_map(
        local,
        mesh=mesh,
        in_specs=(
            P("grp", ("kv", "tp")),
            P("grp"),
            P("kv"),
            P("kv", "tp"),
            P("kv", "tp"),
            P("kv", "tp"),
            P("kv", "tp"),
            P("tp"),
            P("grp", "kv", "tp"),
            P("grp", "kv", "tp"),
            P("tp"),
            P("tp", "kv"),
            P("kv"),
            P("kv", "tp"),
            P("kv", "tp"),
            P("tp", "kv"),
        ),
        out_specs=P("grp", ("kv", "tp")),
        check_vma=False,
    )
```
